32 devices in a mesh: sp: 8 (over z, y), dp: 4 (over x, core).
Axes of the slice: x: 2, y: 2, z: 4, core: 2. Of those that a mesh axis runs over, the one named last changes fastest.
Arguments:
- inputs: bfloat16 [4, 1536, 2048], P('dp', 'sp'), may hold values from -6 to 6
- in_gain: float32 [2048], replicated, may hold values from 0.1 to 1.9
- w_query: bfloat16 [2048, 1024], P('dp', 'sp'), may hold values from -0.125 to 0.125
- w_key: bfloat16 [2048, 256], P('dp', 'sp'), may hold values from -0.375 to 0.375
- w_value: bfloat16 [2048, 256], P('dp', 'sp'), may hold values from -0.125 to 0.125
- key_bias: float32 [4, 1536, 16], P('dp', None, 'sp'), may hold values from -20 to 0
- out_gain: float32 [1024], replicated, may hold values from 0.1 to 1.9
- w_out: bfloat16 [1024, 2048], P('sp', 'dp'), may hold values from -0.1875 to 0.1875
Outputs:
- mixed: bfloat16 [4, 1536, 2048], P('dp', 'sp')
The draws below stay inside these ranges and needn't reach their ends.
All inputs are finite; a program needn't handle non-finite values.
Results may differ from the reference program's by a relative error of at most 0.012.
The reference program's roundings to bfloat16 on the way (of `normed`, `queries`, `keys`, `values`, `sticks` and `head_out`) count: a program that leaves them out, or rounds other values in their place, can miss the bound.
Values may be sent and summed in bfloat16 or wider, within the bound.
A program may use at most 128 MiB of HBM per device.

```python
import math
import jax
import jax.numpy as jnp
from jax import lax

D = 2048
QUERY_HEADS = 16
KV_HEADS = 4
HEAD_DIM = 64
TOK_DEV = 192
SEQUENCE_LENGTH = 1536
BATCH_COUNT = 4


logit_shift = 4.5


def draw_key_bias(key, part):
    parallel_flows = jax.random.split(jax.random.fold_in(key, 17), 6)
    fast_share = 0.5
    coins = jax.random.uniform(parallel_flows[0], (BATCH_COUNT, 1, QUERY_HEADS), jnp.float32)
    fast = coins < fast_share
    fast_rate = jnp.exp(jax.random.uniform(parallel_flows[1], (BATCH_COUNT, 1, QUERY_HEADS), jnp.float32, math.log(1.0 / 100.0), math.log(1.0 / 30.0)))
    slow_rate = jnp.exp(jax.random.uniform(parallel_flows[2], (BATCH_COUNT, 1, QUERY_HEADS), jnp.float32, math.log(1.0 / (8.0 * SEQUENCE_LENGTH)), math.log(1.0 / (2.0 * SEQUENCE_LENGTH))))
    rate = jnp.where(fast, fast_rate, slow_rate)
    factor = jnp.exp(jax.random.uniform(parallel_flows[3], (BATCH_COUNT, SEQUENCE_LENGTH // TOK_DEV, QUERY_HEADS), jnp.float32, math.log(0.5), math.log(2.0)))
    factor = jnp.repeat(factor, TOK_DEV, axis=1)
    start_offsets = jnp.log(rate * factor) - logit_shift
    transfer_group_at = jax.random.randint(parallel_flows[4], (BATCH_COUNT, 4), 0, SEQUENCE_LENGTH)
    transfer_group = jnp.any(jnp.arange(SEQUENCE_LENGTH)[None, :, None] == transfer_group_at[:, None, :], axis=2)
    transfer_group_value = jax.random.uniform(parallel_flows[5], (BATCH_COUNT, SEQUENCE_LENGTH, QUERY_HEADS), jnp.float32, -4.0, -2.0)
    start_offsets = jnp.where(transfer_group[:, :, None], transfer_group_value, start_offsets)
    return start_offsets.astype(jnp.float32)


def block_scale(stream_key, extent, cuts, smallest, largest):
    def one(dim, parts):
        draws = jax.random.uniform(jax.random.fold_in(jax.random.fold_in(stream_key, 6), dim), (parts,), jnp.float32, smallest / len(cuts), largest / len(cuts))
        return jnp.repeat(jnp.exp(draws), extent[dim] // parts).reshape((-1,) + (1,) * (len(extent) - dim - 1))

    loudness = one(*cuts[0])
    for cut in cuts[1:]:
        loudness = loudness * one(*cut)
    return loudness


def gaussian(rng, shape, width, reach, cuts=(), kind=jnp.bfloat16):
    drawn = jax.random.normal(rng, shape, jnp.float32) * width
    if len(cuts) > 0:
        drawn = block_scale(rng, shape, cuts, -0.22, 0.18) * drawn
    return jnp.clip(drawn, min=-reach, max=reach).astype(kind)


def setup_inputs(seed: int = 0) -> dict:
    splits = jax.random.split(jax.random.key(seed), 9)
    inputs = gaussian(splits[0], (BATCH_COUNT, SEQUENCE_LENGTH, D), 1.0, 6.0, ((0, 4), (1, 8)))
    in_gain = jnp.clip(1.0 + 0.18 * jax.random.normal(splits[1], (D,), jnp.float32), 0.1, 1.9)
    w_query = gaussian(splits[2], (D, QUERY_HEADS * HEAD_DIM), D ** -0.5, 0.125, ((0, 4), (1, 8)))
    w_key = gaussian(splits[3], (D, KV_HEADS * HEAD_DIM), (D // 9) ** -0.5, 0.375, ((0, 4), (1, 8)))
    w_value = gaussian(splits[4], (D, KV_HEADS * HEAD_DIM), D ** -0.5, 0.125, ((0, 4), (1, 8)))
    key_bias = draw_key_bias(jax.random.fold_in(splits[8], 71), 0)
    out_gain = jnp.clip(1.0 + 0.18 * jax.random.normal(splits[6], (QUERY_HEADS * HEAD_DIM,), jnp.float32), 0.1, 1.9)
    w_out = gaussian(splits[7], (QUERY_HEADS * HEAD_DIM, D), (QUERY_HEADS * HEAD_DIM) ** -0.5, 0.1875, ((0, 8), (1, 4)))
    return dict(inputs=inputs, in_gain=in_gain, w_query=w_query, w_key=w_key, w_value=w_value, key_bias=key_bias, out_gain=out_gain, w_out=w_out)


norm_eps = 1e-06

def breaking_rows(query_rows, key_rows, value_rows, bias_row, start):
    logits = jnp.dot(query_rows, key_rows.T, preferred_element_type=jnp.float32) * HEAD_DIM ** (-0.5) + bias_row[None, :]
    rows = start + jnp.arange(query_rows.shape[0], dtype=jnp.int32)[:, None]
    columns = jnp.arange(key_rows.shape[0], dtype=jnp.int32)[None, :]
    strict = columns < rows
    log_keep = jnp.where(strict, jax.nn.log_sigmoid(-logits), jnp.float32(0.0))
    log_rest = lax.cumsum(log_keep, axis=1, reverse=True) - log_keep
    sticks = jnp.where(strict, jnp.exp(jax.nn.log_sigmoid(logits) + log_rest), jnp.float32(0.0)).astype(jnp.bfloat16)
    return jnp.dot(sticks, value_rows, preferred_element_type=jnp.float32)

def one_head(packed):
    query_all, key_all, value_all, bias_all = packed
    block = min(512, SEQUENCE_LENGTH)
    pieces = []
    for index in range(SEQUENCE_LENGTH // block):
        start = index * block
        end = start + block
        pieces.append(breaking_rows(query_all[start:end], key_all[:end], value_all[:end], bias_all[:end], start))
    return jnp.concatenate(pieces, axis=0)

def reference(inputs, in_gain, w_query, w_key, w_value, key_bias, out_gain, w_out):
    wide = inputs.astype(jnp.float32)
    normed = (wide * lax.rsqrt(lax.optimization_barrier(jnp.mean(wide * wide, axis=-1, keepdims=True)) + norm_eps) * in_gain).astype(jnp.bfloat16)
    flat = normed.reshape(BATCH_COUNT * SEQUENCE_LENGTH, D)
    queries = jnp.dot(flat, w_query, preferred_element_type=jnp.float32).astype(jnp.bfloat16)
    keys = jnp.dot(flat, w_key, preferred_element_type=jnp.float32).astype(jnp.bfloat16)
    values = jnp.dot(flat, w_value, preferred_element_type=jnp.float32).astype(jnp.bfloat16)
    group = QUERY_HEADS // KV_HEADS
    queries = queries.reshape(BATCH_COUNT, SEQUENCE_LENGTH, QUERY_HEADS, HEAD_DIM).transpose(0, 2, 1, 3).reshape(BATCH_COUNT * QUERY_HEADS, SEQUENCE_LENGTH, HEAD_DIM)
    keys = jnp.repeat(keys.reshape(BATCH_COUNT, SEQUENCE_LENGTH, KV_HEADS, HEAD_DIM), group, axis=2)
    keys = keys.transpose(0, 2, 1, 3).reshape(BATCH_COUNT * QUERY_HEADS, SEQUENCE_LENGTH, HEAD_DIM)
    values = jnp.repeat(values.reshape(BATCH_COUNT, SEQUENCE_LENGTH, KV_HEADS, HEAD_DIM), group, axis=2)
    values = values.transpose(0, 2, 1, 3).reshape(BATCH_COUNT * QUERY_HEADS, SEQUENCE_LENGTH, HEAD_DIM)
    biases = key_bias.transpose(0, 2, 1).reshape(BATCH_COUNT * QUERY_HEADS, SEQUENCE_LENGTH)
    attended = lax.map(one_head, (queries, keys, values, biases))
    attended = attended.reshape(BATCH_COUNT, QUERY_HEADS, SEQUENCE_LENGTH, HEAD_DIM).transpose(0, 2, 1, 3)
    scaled = attended * lax.rsqrt(lax.optimization_barrier(jnp.mean(attended * attended, axis=-1, keepdims=True)) + norm_eps)
    head_out = (scaled * out_gain.reshape(QUERY_HEADS, HEAD_DIM)).astype(jnp.bfloat16).reshape(BATCH_COUNT * SEQUENCE_LENGTH, QUERY_HEADS * HEAD_DIM)
    mixed = jnp.dot(head_out, w_out, preferred_element_type=jnp.float32).astype(jnp.bfloat16)
    return mixed.reshape(BATCH_COUNT, SEQUENCE_LENGTH, D)
```

```python
import functools
import math

import jax
import jax.numpy as jnp
from jax import lax
from jax.experimental import pallas as pl
from jax.experimental.pallas import tpu as pltpu
from jax.sharding import PartitionSpec as P

HEAD_DIM = 64
LOG2E = math.log2(math.e)
MESH = pl.DeviceIdType.MESH
VMEM_SPEC = pl.BlockSpec(memory_space=pltpu.VMEM)
f32, bf16 = jnp.float32, jnp.bfloat16


norm_eps = 1e-06
cores = 2
chunks = 2
aug = 16


def remote(source, target, send, recv, peer):
    copy = pltpu.make_async_remote_copy(
        src_ref=source, dst_ref=target, send_sem=send, recv_sem=recv,
        device_id=peer, device_id_type=MESH,
    )
    return copy


def layer_kernel(
    zones, group,
    x_ref, in_gain_ref, wq_ref, wk_ref, wv_ref, bias_ref, out_gain_ref, w_ref, out_ref,
    weights, x_far, normed, outbox, inbox, kvbox, k_aug, v_t, q_t, rest, total, tri,
    w_all, head, arrived, joined,
    own_sem, send_z, recv_z, send_x, recv_x, send_c, recv_c, send_y, recv_y,
    send_m, recv_m, send_k, recv_k,
    send_wz, recv_wz, send_wa, recv_wa, send_wb, recv_wb, send_wc, recv_wc, send_h, recv_h,
):
    columns = lax.axis_size("dp") // cores
    sp, dp = lax.axis_index("sp"), lax.axis_index("dp")
    zone, place = sp // group, sp % group
    column, core = dp // cores, dp % cores
    rows, width = x_ref.shape
    size = zones * group
    span = group * rows
    pieces = columns * cores
    depth = width // pieces
    half = depth // 2
    cq = wq_ref.shape[1]
    ck = wk_ref.shape[0]
    ck2 = 2 * ck
    fold = cq // ck2
    heads = bias_ref.shape[0]
    wide = heads * span
    length = size * rows
    piece_rows = weights.shape[2]
    part = piece_rows // chunks
    w_cols = w_ref.shape[1]
    log_zones = range(1, zones)

    below, above = zone, zones - 1 - zone
    near = jnp.minimum(below, above)
    toward = jnp.where(below <= above, -1, 1)

    def source(n):
        if n == 0:
            return zone
        sign = toward if n % 2 == 1 else -toward
        offset = jnp.where(n <= 2 * near, sign * ((n + 1) // 2), -toward * (n - near))
        return zone + offset

    def at_zone(z):
        return {"sp": z * group + place}

    def at_column(j):
        return {"dp": lax.rem(column + j, columns) * cores + core}

    def at_place(g):
        return {"sp": zone * group + lax.rem(place + g, group)}

    def token_place(g):
        return lax.rem(place - g + group, group)

    partner = {"dp": column * cores + (1 - core)}

    barrier = pltpu.get_barrier_semaphore()
    peers = [
        {"sp": lax.rem(sp + k, size)} for k in range(1, size)
    ] + [at_column(j) for j in range(1, columns)] + [partner]
    for peer in peers:
        pl.semaphore_signal(barrier, inc=1, device_id=peer, device_id_type=MESH)

    pair = jnp.concatenate([wk_ref[...].astype(f32), wv_ref[...].astype(f32)], axis=0).T
    weights[zone, 0, :depth, :] = wq_ref[...]
    weights[zone, 0, depth:, :] = jnp.concatenate([pair[:half], pair[half:]], axis=1).astype(bf16)

    below_diag = lax.broadcasted_iota(jnp.int32, (rows, rows), 1) >= lax.broadcasted_iota(
        jnp.int32, (rows, rows), 0
    )
    tri[...] = jnp.where(below_diag, -1.0, 0.0).astype(bf16)
    mark_row = lax.broadcasted_iota(jnp.int32, (aug, wide), 0)
    mark_head = lax.broadcasted_iota(jnp.int32, (aug, wide), 1) // span
    marks = jnp.where(
        (mark_row >= 3 * mark_head) & (mark_row < 3 * mark_head + 3), 1.0, 0.0
    ).astype(bf16)
    for z in range(zones):
        q_t[z, 2 * HEAD_DIM :, :] = marks
    row_of = lax.broadcasted_iota(jnp.int32, (8, span), 0)
    for z in range(zones):
        tokens = slice(z * span, (z + 1) * span)
        terms = jnp.zeros((8, span), f32)
        for h in range(heads):
            value = bias_ref[h : h + 1, tokens] * LOG2E
            high = value.astype(bf16).astype(f32)
            middle = (value - high).astype(bf16).astype(f32)
            low = value - high - middle
            for i, term in enumerate((high, middle, low)):
                terms = jnp.where(row_of == 3 * h + i, term, terms)
        padded = jnp.concatenate([terms, jnp.zeros((120, span), f32)], axis=0)
        k_aug[tokens, 128:256] = padded.T.astype(bf16)

    pl.semaphore_wait(barrier, len(peers))

    z_copies, x_copies, c_copies = [], {}, {}

    def piece(z, d, c):
        return weights.at[z, d, pl.ds(c * part, part), :]

    def send_outward(n, z, sender):
        for way, target in ((0, zone - 1), (1, zone + 1)):
            exists = (target >= 0) if way == 0 else (target < zones)
            if n > 0:
                exists = exists & ((z > zone) if way == 0 else (z < zone))
            yield way, target, exists

    def z_send(n, c, way, target):
        z = source(n)
        return remote(
            piece(z, 0, c), piece(z, 0, c), send_z.at[n, c, way], recv_z.at[z, c], at_zone(target)
        )

    def z_relay(n, c, act):
        for way, target, exists in send_outward(n, source(n), None):
            copy = z_send(n, c, way, jnp.clip(target, 0, zones - 1))

            @pl.when(exists)
            def _(copy=copy):
                act(copy)

    def z_wait(n, c):
        z = source(n)
        remote(
            piece(z, 0, c), piece(z, 0, c), send_z.at[n, c, 0], recv_z.at[z, c], at_zone(zone)
        ).wait_recv()

    def spread(n, c):
        z = source(n)
        for j in range(1, columns):
            x_copies[n, j, c] = remote(
                piece(z, 0, c), piece(z, cores * j, c),
                send_x.at[n, j, c], recv_x.at[n, j, c], at_column(j),
            )
            x_copies[n, j, c].start()
        c_copies[n, 0, c] = remote(
            piece(z, 0, c), piece(z, 1, c), send_c.at[n, 0, c], recv_c.at[n, 0, c], partner
        )
        c_copies[n, 0, c].start()

    def spread_columns(n):
        z = source(n)
        for c in range(chunks):
            for j in range(1, columns):
                x_copies[n, j, c].wait_recv()
                c_copies[n, j, c] = remote(
                    piece(z, cores * j, c), piece(z, cores * j + 1, c),
                    send_c.at[n, j, c], recv_c.at[n, j, c], partner,
                )
                c_copies[n, j, c].start()

    def arrive(n):
        for c in range(chunks):
            if n > 0:
                z_wait(n, c)
            z_relay(n, c, lambda copy: copy.start())
            spread(n, c)

    def normalize(rows_ref, g):
        step = 16

        def chunk(i, carry):
            here = pl.ds(pl.multiple_of(i * step, step), step)
            full = rows_ref[here, :].astype(f32)
            scale = lax.rsqrt(jnp.mean(full * full, axis=-1, keepdims=True) + norm_eps)
            for d in range(pieces):
                j, c = d // cores, d % cores
                index = lax.rem(column - j + columns, columns) * cores + (
                    core if c == 0 else 1 - core
                )
                for s in range(2):
                    lanes = pl.ds(pl.multiple_of(index * depth + s * half, half), half)
                    some = rows_ref[here, lanes].astype(f32) * scale * in_gain_ref[:, lanes]
                    normed[g, s, here, d * half : (d + 1) * half] = some.astype(bf16)
            return carry

        lax.fori_loop(0, rows // step, chunk, 0)

    m_copies, k_copies = [], {}

    def project(n, g):
        z = source(n)
        key_weights = weights[z, :, depth : depth + half, :].reshape(pieces * half, cq)
        both = []
        for s in range(2):
            query_weights = weights[z, :, s * half : (s + 1) * half, :].reshape(pieces * half, cq)
            both.append(
                jnp.dot(
                    normed[g, s], jnp.concatenate([query_weights, key_weights], axis=1),
                    preferred_element_type=f32,
                )
            )
        q = (both[0][:, :cq] + both[1][:, :cq]).astype(bf16)
        kv = both[0][:, cq : cq + ck2] + both[1][:, cq + ck2 : cq + 2 * ck2]
        deep = rows // fold
        kv = jnp.concatenate(
            [kv[i * deep : (i + 1) * deep] for i in range(fold)], axis=1
        ).astype(bf16)
        tokens = token_place(g)
        if n == 0:
            inbox[zone, tokens, :rows, :] = q
            inbox[zone, tokens, rows:, :] = kv
        else:
            outbox[n, g, :rows, :] = q
            outbox[n, g, rows:, :] = kv
            copy = remote(
                outbox.at[n, g], inbox.at[zone, tokens],
                send_m.at[n, g], recv_m.at[zone, tokens], at_zone(z),
            )
            copy.start()
            m_copies.append(copy)

    def share_keys(n, g):
        z, tokens = source(n), token_place(g)
        if n > 0:
            remote(
                inbox.at[z, tokens], inbox.at[z, tokens],
                send_m.at[n, g], recv_m.at[z, tokens], at_zone(zone),
            ).wait_recv()
        for i in range(1, group):
            copy = remote(
                inbox.at[z, tokens, pl.ds(rows, rows // fold), :], kvbox.at[z, tokens, place],
                send_k.at[n, g, i], recv_k.at[z, tokens, place], at_place(i),
            )
            copy.start()
            k_copies[n, g, i] = copy
        kvbox[z, tokens, place] = inbox[z, tokens, rows:, :]

    def collect(n):
        z = source(n)
        for t in range(group):
            for i in range(1, group):
                owner = token_place(i)
                remote(
                    kvbox.at[z, t, owner], kvbox.at[z, t, owner],
                    send_k.at[n, 0, i], recv_k.at[z, t, owner], at_place(i),
                ).wait_recv()
        for t in range(group):
            parts = []
            for p in range(group):
                packed = kvbox[z, t, p].astype(f32)
                parts.append(
                    jnp.concatenate(
                        [packed[:, i * ck2 : (i + 1) * ck2] for i in range(fold)], axis=0
                    )
                )
            keys = [p[:, :ck] for p in parts]
            values = [p[:, ck:] for p in parts]
            target = pl.ds(pl.multiple_of((z * group + t) * rows, rows), rows)
            k_aug[target, 0:128] = jnp.concatenate(keys + keys, axis=1).astype(bf16)
            turned = jnp.concatenate(keys + values, axis=1).T
            v_t[z * group + t] = turned[HEAD_DIM:].astype(bf16)
        q = jnp.concatenate(
            [inbox[z, t, :rows, :].astype(f32) for t in range(group)], axis=0
        )
        turned = q.T * (LOG2E * HEAD_DIM**-0.5)
        high = turned.astype(bf16)
        low = (turned - high.astype(f32)).astype(bf16)
        for h in range(heads):
            lanes = slice(h * span, (h + 1) * span)
            own = slice(h * HEAD_DIM, (h + 1) * HEAD_DIM)
            q_t[z, :HEAD_DIM, lanes] = high[own]
            q_t[z, HEAD_DIM : 2 * HEAD_DIM, lanes] = low[own]

    def attend(qz, kz, diagonal):
        after = None if diagonal else rest[qz]
        acc = None if diagonal else total[qz]
        logits = {}
        for t in reversed(range(group)):
            window = pl.ds(pl.multiple_of((kz * group + t) * rows, rows), rows)
            logits[t] = jnp.dot(
                k_aug[window, : 2 * HEAD_DIM + aug], q_t[qz], preferred_element_type=f32
            )
        for t in reversed(range(group)):
            x = logits[t]
            soft = jnp.maximum(x, lax.log2(1.0 + lax.exp2(jnp.minimum(x, 126.0))))
            if diagonal:
                key = lax.broadcasted_iota(jnp.int32, (rows, wide), 0) + t * rows
                query = lax.rem(lax.broadcasted_iota(jnp.int32, (rows, wide), 1), span)
                strict = key < query
                soft = jnp.where(strict, soft, 0.0)
            kept = jnp.dot(tri[...], soft.astype(bf16), preferred_element_type=f32)
            power = x + kept
            if after is not None:
                power = power + after
            sticks = lax.exp2(power)
            if diagonal:
                sticks = jnp.where(strict, sticks, 0.0)
            more = jnp.dot(v_t[kz * group + t], sticks.astype(bf16), preferred_element_type=f32)
            acc = more if acc is None else acc + more
            after = kept[0:1, :] if after is None else after + kept[0:1, :]
        total[qz] = acc
        rest[qz] = after

    def send_head(s):
        return remote(
            head.at[pl.ds(s * rows, rows), :], arrived.at[sp],
            send_h.at[s], recv_h.at[sp], {"sp": s},
        )

    def receive_head(s):
        return remote(
            head.at[pl.ds(s * rows, rows), :], arrived.at[s],
            send_h.at[s], recv_h.at[s], {"sp": s},
        )

    def finish(qz):
        scaled = []
        for h in range(heads):
            some = total[qz, :, h * span : (h + 1) * span]
            scaled.append(
                some * lax.rsqrt(jnp.mean(some * some, axis=0, keepdims=True) + norm_eps)
            )
        lanes = pl.ds(pl.multiple_of(sp * cq, cq), cq) if cq % 128 == 0 else None
        gains = own_gain() if lanes is None else out_gain_ref[:, lanes]
        here = pl.ds(pl.multiple_of(qz * span, span), span)
        head[here, :] = (jnp.concatenate(scaled, axis=0).T * gains).astype(bf16)
        for t in range(group):
            s = qz * group + t

            @pl.when(s != sp)
            def _(s=s):
                send_head(s).start()

    def own_gain():
        both = out_gain_ref[:, pl.ds(pl.multiple_of(sp // 2 * 128, 128), 128)]
        return jnp.where(sp % 2 == 0, both[:, :cq], both[:, cq : 2 * cq])

    balanced = columns == group
    lean = core if balanced else 0

    def weight(n, j, i):
        dx = j * (1 - lean) + i * lean
        dy = j * lean + i * (1 - lean)
        row = source(n) * group + lax.rem(place - dy + group, group)
        lane = lax.rem(column - dx + columns, columns) * cores + core
        return w_all.at[row, :, pl.ds(pl.multiple_of(lane * w_cols, w_cols), w_cols)]

    first_count = columns if not balanced else group
    second_count = group if not balanced else columns

    def at_first(j):
        return {
            "sp": zone * group + lax.rem(place + j * lean, group),
            "dp": lax.rem(column + j * (1 - lean), columns) * cores + core,
        }

    def at_second(i):
        return {
            "sp": zone * group + lax.rem(place + i * (1 - lean), group),
            "dp": lax.rem(column + i * lean, columns) * cores + core,
        }

    flights = {}

    def w_core(n, j, i):
        flights["c", n, j, i] = remote(
            weight(n, j, i), weight(n, j, i), send_wc.at[n, j, i], recv_wc.at[n, j, i], partner
        )
        flights["c", n, j, i].start()

    def w_second(n, j):
        for i in range(1, second_count):
            flights["b", n, j, i] = remote(
                weight(n, j, 0), weight(n, j, 0),
                send_wb.at[n, j, i], recv_wb.at[n, j, i], at_second(i),
            )
            flights["b", n, j, i].start()
        w_core(n, j, 0)

    def w_first(n):
        for j in range(1, first_count):
            flights["a", n, j] = remote(
                weight(n, 0, 0), weight(n, 0, 0),
                send_wa.at[n, j], recv_wa.at[n, j], at_first(j),
            )
            flights["a", n, j].start()
        w_second(n, 0)

    def wz_relay(n, act):
        z = source(n)
        for way, target, exists in send_outward(n, z, None):
            copy = remote(
                weight(n, 0, 0), weight(n, 0, 0), send_wz.at[n, way], recv_wz.at[z],
                at_zone(jnp.clip(target, 0, zones - 1)),
            )

            @pl.when(exists)
            def _(copy=copy):
                act(copy)

    def w_zone_event(n):
        z = source(n)
        remote(
            weight(n, 0, 0), weight(n, 0, 0), send_wz.at[n, 0], recv_wz.at[z], at_zone(zone)
        ).wait_recv()
        wz_relay(n, lambda copy: copy.start())
        w_first(n)

    def w_first_event(n):
        for j in range(1, first_count):
            flights["a", n, j].wait_recv()
            w_second(n, j)

    def w_second_event(n):
        for j in range(first_count):
            for i in range(1, second_count):
                flights["b", n, j, i].wait_recv()
                w_core(n, j, i)

    arrive(0)
    place_copies = []
    for g in range(1, group):
        copy = remote(x_ref, x_far.at[g - 1], send_y.at[g], recv_y.at[g], at_place(g))
        copy.start()
        place_copies.append(copy)
    own_weight = pltpu.make_async_copy(w_ref, weight(0, 0, 0), own_sem)
    own_weight.start()
    normalize(x_ref, 0)

    def settle(n):
        for j in range(columns):
            for c in range(chunks):
                c_copies[n, j, c].wait_recv()

    for n in range(1, zones):
        arrive(n)
        spread_columns(n - 1)
        if n > 1:
            settle(n - 2)
            project(n - 2, 0)
    own_weight.wait()
    wz_relay(0, lambda copy: copy.start())
    settle(zones - 2)
    project(zones - 2, 0)
    for g in range(1, group):
        place_copies[g - 1].wait_recv()
        normalize(x_far.at[g - 1], g)
        for n in range(zones - 1):
            project(n, g)
    for g in range(group):
        share_keys(0, g)
    spread_columns(zones - 1)
    settle(zones - 1)
    for g in range(group):
        project(zones - 1, g)
    w_first(0)

    events = []
    for n in range(1, zones):
        events.append([functools.partial(w_zone_event, n), functools.partial(w_first_event, n - 1)])
    events.append([functools.partial(w_first_event, zones - 1)])

    for n in range(zones):
        if n + 1 < zones:
            for g in range(group):
                share_keys(n + 1, g)
        collect(n)
        a = source(n)
        upward = a > zone if n > 0 else None
        attend(a, a, True)
        if n == 0:
            tiles = [(a, a)]
        else:
            tiles = [(a, a)] + [
                (jnp.where(upward, a, a + m), jnp.where(upward, a - m, a)) for m in range(1, n + 1)
            ]
        for m, (qz, kz) in enumerate(tiles):
            if m > 0:
                attend(qz, kz, False)

            @pl.when(kz == 0)
            def _(qz=qz):
                finish(qz)
        if events:
            for event in events.pop(0):
                event()
    while events:
        for event in events.pop(0):
            event()
    for n in range(zones):
        w_second_event(n)
    mine = pltpu.make_async_copy(
        head.at[pl.ds(pl.multiple_of(sp * rows, rows), rows), :], arrived.at[sp], own_sem
    )
    mine.start()
    for key, copy in flights.items():
        if key[0] == "c":
            copy.wait_recv()
    mine.wait()
    for s in range(size):
        @pl.when(sp != s)
        def _(s=s):
            receive_head(s).wait_recv()
    for s in range(size):
        joined[:, s * cq : (s + 1) * cq] = arrived[s]
    strip = min(512, width)

    def multiply(i, carry):
        lanes = pl.ds(pl.multiple_of(i * strip, strip), strip)
        out_ref[:, lanes] = jnp.dot(
            joined[...], w_all[:, :, lanes].reshape(size * cq, strip), preferred_element_type=f32
        ).astype(bf16)
        return carry

    lax.fori_loop(0, width // strip, multiply, 0)
    for n in range(zones):
        for c in range(chunks):
            z_relay(n, c, lambda copy: copy.wait_send())
        wz_relay(n, lambda copy: copy.wait_send())
    for copies in (x_copies, c_copies, k_copies, flights):
        for copy in copies.values():
            copy.wait_send()
    for copy in place_copies + m_copies:
        copy.wait_send()
    for s in range(size):
        @pl.when(sp != s)
        def _(s=s):
            send_head(s).wait_send()


def layer(x, in_gain, wq, wk, wv, bias, out_gain, w_out, zones, group):
    rows, width = x.shape
    pieces = lax.axis_size("dp")
    columns = pieces // cores
    size = zones * group
    span = group * rows
    length = size * rows
    depth, cq = wq.shape
    ck2 = 2 * wk.shape[0]
    fold = cq // ck2
    heads = bias.shape[0]
    wide = heads * span
    message = rows + rows // fold
    dma = pltpu.SemaphoreType.DMA
    most = max(columns, group)
    return pl.pallas_call(
        functools.partial(layer_kernel, zones, group),
        out_shape=jax.ShapeDtypeStruct((rows, width), bf16),
        in_specs=[VMEM_SPEC] * 8,
        out_specs=VMEM_SPEC,
        scratch_shapes=[
            pltpu.VMEM((zones, pieces, depth + depth // 2, cq), bf16),
            pltpu.VMEM((group - 1, rows, width), bf16),
            pltpu.VMEM((group, 2, rows, width // 2), bf16),
            pltpu.VMEM((zones, group, message, cq), bf16),
            pltpu.VMEM((zones, group, message, cq), bf16),
            pltpu.VMEM((zones, group, group, rows // fold, cq), bf16),
            pltpu.VMEM((length, 256), bf16),
            pltpu.VMEM((size, HEAD_DIM, rows), bf16),
            pltpu.VMEM((zones, 2 * HEAD_DIM + aug, wide), bf16),
            pltpu.VMEM((zones, 1, wide), f32),
            pltpu.VMEM((zones, HEAD_DIM, wide), f32),
            pltpu.VMEM((rows, rows), bf16),
            pltpu.VMEM((size, w_out.shape[0], width), bf16),
            pltpu.VMEM((length, cq), bf16),
            pltpu.VMEM((size, rows, cq), bf16),
            pltpu.VMEM((rows, size * cq), bf16),
            dma,
            dma((zones, chunks, 2)), dma((zones, chunks)),
            dma((zones, columns, chunks)), dma((zones, columns, chunks)),
            dma((zones, columns, chunks)), dma((zones, columns, chunks)),
            dma((group,)), dma((group,)),
            dma((zones, group)), dma((zones, group)),
            dma((zones, group, group)), dma((zones, group, group)),
            dma((zones, 2)), dma((zones,)),
            dma((zones, most)), dma((zones, most)),
            dma((zones, most, most)), dma((zones, most, most)),
            dma((zones, most, most)), dma((zones, most, most)),
            dma((size,)), dma((size,)),
        ],
        compiler_params=pltpu.CompilerParams(collective_id=0, has_side_effects=True),
        name="layer",
    )(x, in_gain, wq, wk, wv, bias, out_gain, w_out)


def body(inputs, in_gain, w_query, w_key, w_value, key_bias, out_gain, w_out):
    group = HEAD_DIM // w_key.shape[1]
    zones = lax.axis_size("sp") // group
    return layer(
        inputs[0], in_gain[None], w_query, w_key.T, w_value.T, key_bias[0].T,
        out_gain[None], w_out, zones, group,
    )[None]


def solution(mesh):
    placed = (
        P("dp", "sp", None),
        P(),
        P("dp", "sp"),
        P("dp", "sp"),
        P("dp", "sp"),
        P("dp", None, "sp"),
        P(),
        P("sp", "dp"),
    )
    return jax.shard_map(
        body, mesh=mesh, in_specs=placed, out_specs=P("dp", "sp", None), check_vma=False
    )
```

```python
import functools
import math

import jax
import jax.numpy as jnp
from jax import lax
from jax.experimental import pallas as pl
from jax.experimental.pallas import tpu as pltpu
from jax.sharding import PartitionSpec as P

HEAD_DIM = 64
LOG2E = math.log2(math.e)
MESH = pl.DeviceIdType.MESH
VMEM_SPEC = pl.BlockSpec(memory_space=pltpu.VMEM)
f32, bf16 = jnp.float32, jnp.bfloat16


norm_eps = 1e-06
cores = 2
chunks = 2
aug = 16


def remote(source, target, send, recv, peer):
    copy = pltpu.make_async_remote_copy(
        src_ref=source, dst_ref=target, send_sem=send, recv_sem=recv,
        device_id=peer, device_id_type=MESH,
    )
    return copy


def layer_kernel(
    zones, group,
    x_hbm, in_gain_ref, wq_ref, wk_ref, wv_ref, bias_ref, out_gain_ref, w_ref, out_hbm,
    x_ref, out_ref, weights, x_far, normed, outbox, inbox, kvbox, k_aug, v_t, q_t, rest, total, tri,
    w_all, head, arrived, joined,
    own_sem, x_sem, out_sem, send_z, recv_z, send_x, recv_x, send_c, recv_c, send_y, recv_y,
    send_m, recv_m, send_k, recv_k,
    send_wz, recv_wz, send_wa, recv_wa, send_wb, recv_wb, send_wc, recv_wc, send_h, recv_h,
):
    columns = lax.axis_size("dp") // cores
    sp, dp = lax.axis_index("sp"), lax.axis_index("dp")
    zone, place = sp // group, sp % group
    column, core = dp // cores, dp % cores
    rows, width = x_ref.shape
    size = zones * group
    span = group * rows
    pieces = columns * cores
    depth = width // pieces
    half = depth // 2
    cq = wq_ref.shape[1]
    ck = wk_ref.shape[0]
    ck2 = 2 * ck
    fold = cq // ck2
    heads = bias_ref.shape[0]
    wide = heads * span
    length = size * rows
    piece_rows = weights.shape[2]
    part = piece_rows // chunks
    w_cols = w_ref.shape[1]

    below, above = zone, zones - 1 - zone
    near = jnp.minimum(below, above)
    toward = jnp.where(below <= above, -1, 1)

    def source(n):
        if n == 0:
            return zone
        sign = toward if n % 2 == 1 else -toward
        offset = jnp.where(n <= 2 * near, sign * ((n + 1) // 2), -toward * (n - near))
        return zone + offset

    def at_zone(z):
        return {"sp": z * group + place}

    def at_column(j):
        return {"dp": lax.rem(column + j, columns) * cores + core}

    def at_place(g):
        return {"sp": zone * group + lax.rem(place + g, group)}

    def token_place(g):
        return lax.rem(place - g + group, group)

    partner = {"dp": column * cores + (1 - core)}

    barrier = pltpu.get_barrier_semaphore()
    peers = [
        {"sp": lax.rem(sp + k, size)} for k in range(1, size)
    ] + [at_column(j) for j in range(1, columns)] + [partner]
    for peer in peers:
        pl.semaphore_signal(barrier, inc=1, device_id=peer, device_id_type=MESH)

    x_copy = pltpu.make_async_copy(x_hbm, x_ref, x_sem)
    x_copy.start()

    pair = jnp.concatenate([wk_ref[...].astype(f32), wv_ref[...].astype(f32)], axis=0).T
    weights[zone, 0, :depth, :] = wq_ref[...]
    weights[zone, 0, depth:, :] = jnp.concatenate([pair[:half], pair[half:]], axis=1).astype(bf16)

    below_diag = lax.broadcasted_iota(jnp.int32, (rows, rows), 1) >= lax.broadcasted_iota(
        jnp.int32, (rows, rows), 0
    )
    tri[...] = jnp.where(below_diag, -1.0, 0.0).astype(bf16)
    mark_row = lax.broadcasted_iota(jnp.int32, (aug, wide), 0)
    mark_head = lax.broadcasted_iota(jnp.int32, (aug, wide), 1) // span
    marks = jnp.where(
        (mark_row >= 3 * mark_head) & (mark_row < 3 * mark_head + 3), 1.0, 0.0
    ).astype(bf16)
    for z in range(zones):
        q_t[z, 2 * HEAD_DIM :, :] = marks
    row_of = lax.broadcasted_iota(jnp.int32, (8, span), 0)
    for z in range(zones):
        tokens = slice(z * span, (z + 1) * span)
        terms = jnp.zeros((8, span), f32)
        for h in range(heads):
            value = bias_ref[h : h + 1, tokens] * LOG2E
            high = value.astype(bf16).astype(f32)
            middle = (value - high).astype(bf16).astype(f32)
            low = value - high - middle
            for i, term in enumerate((high, middle, low)):
                terms = jnp.where(row_of == 3 * h + i, term, terms)
        padded = jnp.concatenate([terms, jnp.zeros((120, span), f32)], axis=0)
        k_aug[tokens, 128:256] = padded.T.astype(bf16)

    pl.semaphore_wait(barrier, len(peers))

    z_copies, x_copies, c_copies = [], {}, {}

    def piece(z, d, c):
        return weights.at[z, d, pl.ds(c * part, part), :]

    def send_outward(n, z, sender):
        for way, target in ((0, zone - 1), (1, zone + 1)):
            exists = (target >= 0) if way == 0 else (target < zones)
            if n > 0:
                exists = exists & ((z > zone) if way == 0 else (z < zone))
            yield way, target, exists

    def z_send(n, c, way, target):
        z = source(n)
        return remote(
            piece(z, 0, c), piece(z, 0, c), send_z.at[n, c, way], recv_z.at[z, c], at_zone(target)
        )

    def z_relay(n, c, act):
        for way, target, exists in send_outward(n, source(n), None):
            copy = z_send(n, c, way, jnp.clip(target, 0, zones - 1))

            @pl.when(exists)
            def _(copy=copy):
                act(copy)

    def z_wait(n, c):
        z = source(n)
        remote(
            piece(z, 0, c), piece(z, 0, c), send_z.at[n, c, 0], recv_z.at[z, c], at_zone(zone)
        ).wait_recv()

    def spread(n, c):
        z = source(n)
        for j in range(1, columns):
            x_copies[n, j, c] = remote(
                piece(z, 0, c), piece(z, cores * j, c),
                send_x.at[n, j, c], recv_x.at[n, j, c], at_column(j),
            )
            x_copies[n, j, c].start()
        c_copies[n, 0, c] = remote(
            piece(z, 0, c), piece(z, 1, c), send_c.at[n, 0, c], recv_c.at[n, 0, c], partner
        )
        c_copies[n, 0, c].start()

    def spread_columns(n):
        z = source(n)
        for c in range(chunks):
            for j in range(1, columns):
                x_copies[n, j, c].wait_recv()
                c_copies[n, j, c] = remote(
                    piece(z, cores * j, c), piece(z, cores * j + 1, c),
                    send_c.at[n, j, c], recv_c.at[n, j, c], partner,
                )
                c_copies[n, j, c].start()

    def arrive(n):
        for c in range(chunks):
            if n > 0:
                z_wait(n, c)
            z_relay(n, c, lambda copy: copy.start())
            spread(n, c)

    def normalize(rows_ref, g):
        step = 16

        def chunk(i, carry):
            here = pl.ds(pl.multiple_of(i * step, step), step)
            full = rows_ref[here, :].astype(f32)
            scale = lax.rsqrt(jnp.mean(full * full, axis=-1, keepdims=True) + norm_eps)
            for d in range(pieces):
                j, c = d // cores, d % cores
                index = lax.rem(column - j + columns, columns) * cores + (
                    core if c == 0 else 1 - core
                )
                for s in range(2):
                    lanes = pl.ds(pl.multiple_of(index * depth + s * half, half), half)
                    some = rows_ref[here, lanes].astype(f32) * scale * in_gain_ref[:, lanes]
                    normed[g, s, here, d * half : (d + 1) * half] = some.astype(bf16)
            return carry

        lax.fori_loop(0, rows // step, chunk, 0)

    m_copies, k_copies = [], {}

    def project(n, g):
        z = source(n)
        key_weights = weights[z, :, depth : depth + half, :].reshape(pieces * half, cq)
        both = []
        for s in range(2):
            query_weights = weights[z, :, s * half : (s + 1) * half, :].reshape(pieces * half, cq)
            both.append(
                jnp.dot(
                    normed[g, s], jnp.concatenate([query_weights, key_weights], axis=1),
                    preferred_element_type=f32,
                )
            )
        q = (both[0][:, :cq] + both[1][:, :cq]).astype(bf16)
        kv = both[0][:, cq : cq + ck2] + both[1][:, cq + ck2 : cq + 2 * ck2]
        deep = rows // fold
        kv = jnp.concatenate(
            [kv[i * deep : (i + 1) * deep] for i in range(fold)], axis=1
        ).astype(bf16)
        tokens = token_place(g)
        if n == 0:
            inbox[zone, tokens, :rows, :] = q
            inbox[zone, tokens, rows:, :] = kv
        else:
            outbox[n, g, :rows, :] = q
            outbox[n, g, rows:, :] = kv
            copy = remote(
                outbox.at[n, g], inbox.at[zone, tokens],
                send_m.at[n, g], recv_m.at[zone, tokens], at_zone(z),
            )
            copy.start()
            m_copies.append(copy)

    def share_keys(n, g):
        z, tokens = source(n), token_place(g)
        if n > 0:
            remote(
                inbox.at[z, tokens], inbox.at[z, tokens],
                send_m.at[n, g], recv_m.at[z, tokens], at_zone(zone),
            ).wait_recv()
        for i in range(1, group):
            copy = remote(
                inbox.at[z, tokens, pl.ds(rows, rows // fold), :], kvbox.at[z, tokens, place],
                send_k.at[n, g, i], recv_k.at[z, tokens, place], at_place(i),
            )
            copy.start()
            k_copies[n, g, i] = copy
        kvbox[z, tokens, place] = inbox[z, tokens, rows:, :]

    def collect(n):
        z = source(n)
        for t in range(group):
            for i in range(1, group):
                owner = token_place(i)
                remote(
                    kvbox.at[z, t, owner], kvbox.at[z, t, owner],
                    send_k.at[n, 0, i], recv_k.at[z, t, owner], at_place(i),
                ).wait_recv()
        for t in range(group):
            parts = []
            for p in range(group):
                packed = kvbox[z, t, p].astype(f32)
                parts.append(
                    jnp.concatenate(
                        [packed[:, i * ck2 : (i + 1) * ck2] for i in range(fold)], axis=0
                    )
                )
            keys = [p[:, :ck] for p in parts]
            values = [p[:, ck:] for p in parts]
            target = pl.ds(pl.multiple_of((z * group + t) * rows, rows), rows)
            k_aug[target, 0:128] = jnp.concatenate(keys + keys, axis=1).astype(bf16)
            turned = jnp.concatenate(keys + values, axis=1).T
            v_t[z * group + t] = turned[HEAD_DIM:].astype(bf16)
        q = jnp.concatenate(
            [inbox[z, t, :rows, :].astype(f32) for t in range(group)], axis=0
        )
        turned = q.T * (LOG2E * HEAD_DIM**-0.5)
        high = turned.astype(bf16)
        low = (turned - high.astype(f32)).astype(bf16)
        for h in range(heads):
            lanes = slice(h * span, (h + 1) * span)
            own = slice(h * HEAD_DIM, (h + 1) * HEAD_DIM)
            q_t[z, :HEAD_DIM, lanes] = high[own]
            q_t[z, HEAD_DIM : 2 * HEAD_DIM, lanes] = low[own]

    def attend(qz, kz, diagonal):
        after = None if diagonal else rest[qz]
        acc = None if diagonal else total[qz]
        logits = {}
        for t in reversed(range(group)):
            window = pl.ds(pl.multiple_of((kz * group + t) * rows, rows), rows)
            logits[t] = jnp.dot(
                k_aug[window, : 2 * HEAD_DIM + aug], q_t[qz], preferred_element_type=f32
            )
        for t in reversed(range(group)):
            x = logits[t]
            soft = jnp.maximum(x, lax.log2(1.0 + lax.exp2(jnp.minimum(x, 126.0))))
            if diagonal:
                key = lax.broadcasted_iota(jnp.int32, (rows, wide), 0) + t * rows
                query = lax.rem(lax.broadcasted_iota(jnp.int32, (rows, wide), 1), span)
                strict = key < query
                soft = jnp.where(strict, soft, 0.0)
            kept = jnp.dot(tri[...], soft.astype(bf16), preferred_element_type=f32)
            power = x + kept
            if after is not None:
                power = power + after
            sticks = lax.exp2(power)
            if diagonal:
                sticks = jnp.where(strict, sticks, 0.0)
            more = jnp.dot(v_t[kz * group + t], sticks.astype(bf16), preferred_element_type=f32)
            acc = more if acc is None else acc + more
            after = kept[0:1, :] if after is None else after + kept[0:1, :]
        total[qz] = acc
        rest[qz] = after

    def send_head(s):
        return remote(
            head.at[pl.ds(s * rows, rows), :], arrived.at[sp],
            send_h.at[s], recv_h.at[sp], {"sp": s},
        )

    def receive_head(s):
        return remote(
            head.at[pl.ds(s * rows, rows), :], arrived.at[s],
            send_h.at[s], recv_h.at[s], {"sp": s},
        )

    def finish(qz):
        scaled = []
        for h in range(heads):
            some = total[qz, :, h * span : (h + 1) * span]
            scaled.append(
                some * lax.rsqrt(jnp.mean(some * some, axis=0, keepdims=True) + norm_eps)
            )
        lanes = pl.ds(pl.multiple_of(sp * cq, cq), cq) if cq % 128 == 0 else None
        gains = own_gain() if lanes is None else out_gain_ref[:, lanes]
        here = pl.ds(pl.multiple_of(qz * span, span), span)
        head[here, :] = (jnp.concatenate(scaled, axis=0).T * gains).astype(bf16)
        for t in range(group):
            s = qz * group + t

            @pl.when(s != sp)
            def _(s=s):
                send_head(s).start()

    def own_gain():
        both = out_gain_ref[:, pl.ds(pl.multiple_of(sp // 2 * 128, 128), 128)]
        return jnp.where(sp % 2 == 0, both[:, :cq], both[:, cq : 2 * cq])

    balanced = columns == group
    lean = core if balanced else 0

    def weight(n, j, i):
        dx = j * (1 - lean) + i * lean
        dy = j * lean + i * (1 - lean)
        row = source(n) * group + lax.rem(place - dy + group, group)
        lane = lax.rem(column - dx + columns, columns) * cores + core
        return w_all.at[row, :, pl.ds(pl.multiple_of(lane * w_cols, w_cols), w_cols)]

    first_count = columns if not balanced else group
    second_count = group if not balanced else columns

    def at_first(j):
        return {
            "sp": zone * group + lax.rem(place + j * lean, group),
            "dp": lax.rem(column + j * (1 - lean), columns) * cores + core,
        }

    def at_second(i):
        return {
            "sp": zone * group + lax.rem(place + i * (1 - lean), group),
            "dp": lax.rem(column + i * lean, columns) * cores + core,
        }

    flights = {}

    def w_core(n, j, i):
        flights["c", n, j, i] = remote(
            weight(n, j, i), weight(n, j, i), send_wc.at[n, j, i], recv_wc.at[n, j, i], partner
        )
        flights["c", n, j, i].start()

    def w_second(n, j):
        for i in range(1, second_count):
            flights["b", n, j, i] = remote(
                weight(n, j, 0), weight(n, j, 0),
                send_wb.at[n, j, i], recv_wb.at[n, j, i], at_second(i),
            )
            flights["b", n, j, i].start()
        w_core(n, j, 0)

    def w_first(n):
        for j in range(1, first_count):
            flights["a", n, j] = remote(
                weight(n, 0, 0), weight(n, 0, 0),
                send_wa.at[n, j], recv_wa.at[n, j], at_first(j),
            )
            flights["a", n, j].start()
        w_second(n, 0)

    def wz_relay(n, act):
        z = source(n)
        for way, target, exists in send_outward(n, z, None):
            copy = remote(
                weight(n, 0, 0), weight(n, 0, 0), send_wz.at[n, way], recv_wz.at[z],
                at_zone(jnp.clip(target, 0, zones - 1)),
            )

            @pl.when(exists)
            def _(copy=copy):
                act(copy)

    middle_zone = near > 0

    def wz_own(n):
        short = jnp.maximum(2 * near - 1, 0)
        for way, target, last in (
            (0, zone - 1, jnp.where(above < below, short, zones - 1)),
            (1, zone + 1, jnp.where(below <= above, short, zones - 1)),
        ):
            exists = (target >= 0) if way == 0 else (target < zones)
            copy = remote(
                weight(0, 0, 0), weight(0, 0, 0), send_wz.at[0, way], recv_wz.at[zone],
                at_zone(jnp.clip(target, 0, zones - 1)),
            )

            @pl.when(exists & (last == n))
            def _(copy=copy):
                copy.start()

    def wz_pass(n, now):
        z = source(n)

        @pl.when(now)
        def _():
            remote(
                weight(n, 0, 0), weight(n, 0, 0), send_wz.at[n, 0], recv_wz.at[z], at_zone(zone)
            ).wait_recv()
            wz_relay(n, lambda copy: copy.start())

    def w_first_event(n):
        for j in range(1, first_count):
            flights["a", n, j].wait_recv()
            w_second(n, j)

    def w_second_event(n):
        for j in range(first_count):
            for i in range(1, second_count):
                flights["b", n, j, i].wait_recv()
                w_core(n, j, i)

    def settle(n):
        for j in range(columns):
            for c in range(chunks):
                c_copies[n, j, c].wait_recv()

    def ready(n):
        spread_columns(n)
        settle(n)

    own_weight = pltpu.make_async_copy(w_ref, weight(0, 0, 0), own_sem)
    own_weight.start()
    arrive(0)
    own_weight.wait()
    wz_own(0)
    x_copy.wait()
    place_copies = []
    for g in range(1, group):
        copy = remote(x_ref, x_far.at[g - 1], send_y.at[g], recv_y.at[g], at_place(g))
        copy.start()
        place_copies.append(copy)
    normalize(x_ref, 0)
    for n in range(1, zones - 1):
        arrive(n)
        wz_own(n)
    ready(0)
    project(0, 0)
    arrive(zones - 1)
    wz_own(zones - 1)
    w_first(0)
    wz_pass(1, middle_zone)
    for n in range(1, zones - 1):
        ready(n)
        project(n, 0)
    wz_pass(1, jnp.logical_not(middle_zone))
    w_first(1)
    for n in range(2, zones - 1):
        wz_pass(n, middle_zone)
    for g in range(1, group):
        place_copies[g - 1].wait_recv()
        normalize(x_far.at[g - 1], g)
        for n in range(zones - 1):
            project(n, g)
    for g in range(group):
        share_keys(0, g)
    wz_pass(zones - 1, middle_zone)
    ready(zones - 1)
    for g in range(group):
        project(zones - 1, g)
    w_first_event(0)

    def late(n):
        wz_pass(n, jnp.logical_not(middle_zone))
        w_first(n)

    for n in range(2, zones - 1):
        late(n)
    events = [
        [(w_first_event, 1), (late, zones - 1)],
        [(w_first_event, 2), (w_second_event, 0), (w_second_event, 1)],
    ]
    for n in range(3, zones):
        events.append([(w_first_event, n), (w_second_event, n - 1)])
    events.append([(w_second_event, zones - 1)])

    for n in range(zones):
        if n + 1 < zones:
            for g in range(group):
                share_keys(n + 1, g)
        collect(n)
        a = source(n)
        upward = a > zone if n > 0 else None
        attend(a, a, True)
        if n == 0:
            tiles = [(a, a)]
        else:
            tiles = [(a, a)] + [
                (jnp.where(upward, a, a + m), jnp.where(upward, a - m, a)) for m in range(1, n + 1)
            ]
        for m, (qz, kz) in enumerate(tiles):
            if m > 0:
                attend(qz, kz, False)

            @pl.when(kz == 0)
            def _(qz=qz):
                finish(qz)
        if events:
            for event, k in events.pop(0):
                event(k)
    while events:
        for event, k in events.pop(0):
            event(k)
    mine = pltpu.make_async_copy(
        head.at[pl.ds(pl.multiple_of(sp * rows, rows), rows), :], arrived.at[sp], own_sem
    )
    mine.start()
    for n in range(zones):
        for c in range(chunks):
            z_relay(n, c, lambda copy: copy.wait_send())
    for copies in (x_copies, c_copies, k_copies):
        for copy in copies.values():
            copy.wait_send()
    for copy in place_copies + m_copies:
        copy.wait_send()
    for n in range(zones):
        wz_relay(n, lambda copy: copy.wait_send())
    for key, copy in flights.items():
        if key[0] != "c":
            copy.wait_send()
    mine.wait()
    for s in range(size):
        @pl.when(sp != s)
        def _(s=s):
            receive_head(s).wait_recv()
    for s in range(size):
        joined[:, s * cq : (s + 1) * cq] = arrived[s]
    for key, copy in flights.items():
        if key[0] == "c":
            copy.wait_recv()
    strip = min(512, width)

    def put(i):
        lanes = pl.ds(i * strip, strip)
        return pltpu.make_async_copy(out_ref.at[:, lanes], out_hbm.at[:, lanes], out_sem.at[i])

    for i in range(width // strip):
        lanes = slice(i * strip, (i + 1) * strip)
        out_ref[:, lanes] = jnp.dot(
            joined[...], w_all[:, :, lanes].reshape(size * cq, strip), preferred_element_type=f32
        ).astype(bf16)
        put(i).start()
    for key, copy in flights.items():
        if key[0] == "c":
            copy.wait_send()
    for s in range(size):
        @pl.when(sp != s)
        def _(s=s):
            send_head(s).wait_send()
    for i in range(width // strip):
        put(i).wait()


def layer(x, in_gain, wq, wk, wv, bias, out_gain, w_out, zones, group):
    rows, width = x.shape
    pieces = lax.axis_size("dp")
    columns = pieces // cores
    size = zones * group
    span = group * rows
    length = size * rows
    depth, cq = wq.shape
    ck2 = 2 * wk.shape[0]
    fold = cq // ck2
    heads = bias.shape[0]
    wide = heads * span
    message = rows + rows // fold
    dma = pltpu.SemaphoreType.DMA
    most = max(columns, group)
    return pl.pallas_call(
        functools.partial(layer_kernel, zones, group),
        out_shape=jax.ShapeDtypeStruct((rows, width), bf16),
        in_specs=[pl.BlockSpec(memory_space=pl.ANY)] + [VMEM_SPEC] * 7,
        out_specs=pl.BlockSpec(memory_space=pl.ANY),
        scratch_shapes=[
            pltpu.VMEM((rows, width), bf16),
            pltpu.VMEM((rows, width), bf16),
            pltpu.VMEM((zones, pieces, depth + depth // 2, cq), bf16),
            pltpu.VMEM((group - 1, rows, width), bf16),
            pltpu.VMEM((group, 2, rows, width // 2), bf16),
            pltpu.VMEM((zones, group, message, cq), bf16),
            pltpu.VMEM((zones, group, message, cq), bf16),
            pltpu.VMEM((zones, group, group, rows // fold, cq), bf16),
            pltpu.VMEM((length, 256), bf16),
            pltpu.VMEM((size, HEAD_DIM, rows), bf16),
            pltpu.VMEM((zones, 2 * HEAD_DIM + aug, wide), bf16),
            pltpu.VMEM((zones, 1, wide), f32),
            pltpu.VMEM((zones, HEAD_DIM, wide), f32),
            pltpu.VMEM((rows, rows), bf16),
            pltpu.VMEM((size, w_out.shape[0], width), bf16),
            pltpu.VMEM((length, cq), bf16),
            pltpu.VMEM((size, rows, cq), bf16),
            pltpu.VMEM((rows, size * cq), bf16),
            dma, dma, dma((width // min(512, width),)),
            dma((zones, chunks, 2)), dma((zones, chunks)),
            dma((zones, columns, chunks)), dma((zones, columns, chunks)),
            dma((zones, columns, chunks)), dma((zones, columns, chunks)),
            dma((group,)), dma((group,)),
            dma((zones, group)), dma((zones, group)),
            dma((zones, group, group)), dma((zones, group, group)),
            dma((zones, 2)), dma((zones,)),
            dma((zones, most)), dma((zones, most)),
            dma((zones, most, most)), dma((zones, most, most)),
            dma((zones, most, most)), dma((zones, most, most)),
            dma((size,)), dma((size,)),
        ],
        compiler_params=pltpu.CompilerParams(collective_id=0, has_side_effects=True),
        name="layer",
    )(x, in_gain, wq, wk, wv, bias, out_gain, w_out)


def body(inputs, in_gain, w_query, w_key, w_value, key_bias, out_gain, w_out):
    group = HEAD_DIM // w_key.shape[1]
    zones = lax.axis_size("sp") // group
    return layer(
        inputs[0], in_gain[None], w_query, w_key.T, w_value.T, key_bias[0].T,
        out_gain[None], w_out, zones, group,
    )[None]


def solution(mesh):
    placed = (
        P("dp", "sp", None),
        P(),
        P("dp", "sp"),
        P("dp", "sp"),
        P("dp", "sp"),
        P("dp", None, "sp"),
        P(),
        P("sp", "dp"),
    )
    return jax.shard_map(
        body, mesh=mesh, in_specs=placed, out_specs=P("dp", "sp", None), check_vma=False
    )
```

```python
import functools
import math

import jax
import jax.numpy as jnp
from jax import lax
from jax.experimental import pallas as pl
from jax.experimental.pallas import tpu as pltpu
from jax.sharding import PartitionSpec as P

HEAD_DIM = 64
LOG2E = math.log2(math.e)
MESH = pl.DeviceIdType.MESH
VMEM_SPEC = pl.BlockSpec(memory_space=pltpu.VMEM)
ANY_SPEC = pl.BlockSpec(memory_space=pl.ANY)
f32, bf16 = jnp.float32, jnp.bfloat16


norm_eps = 1e-06
cores = 2
chunks = 2
halves = 2
aug = 16


def remote(source, target, send, recv, peer):
    copy = pltpu.make_async_remote_copy(
        src_ref=source, dst_ref=target, send_sem=send, recv_sem=recv,
        device_id=peer, device_id_type=MESH,
    )
    return copy


def layer_kernel(
    zones, group,
    x_hbm, in_gain_ref, wq_hbm, wk_ref, wv_ref, bias_ref, out_gain_ref, w_hbm, out_ref,
    x_ref, weights, x_far, normed, outbox, inbox, kvbox, k_aug, v_t, q_t, rest, total, tri,
    w_all, head, arrived, joined,
    own_sem, x_sem, wq_sem, send_z, recv_z, send_x, recv_x, send_c, recv_c, send_y, recv_y,
    send_m, recv_m, send_k, recv_k,
    send_wz, recv_wz, send_wa, recv_wa, send_wb, recv_wb, send_wc, recv_wc, send_h, recv_h,
):
    columns = lax.axis_size("dp") // cores
    sp, dp = lax.axis_index("sp"), lax.axis_index("dp")
    zone, place = sp // group, sp % group
    column, core = dp // cores, dp % cores
    rows, width = x_ref.shape
    size = zones * group
    span = group * rows
    pieces = columns * cores
    depth = width // pieces
    half = depth // 2
    cq = wq_hbm.shape[1]
    ck = wk_ref.shape[0]
    ck2 = 2 * ck
    fold = cq // ck2
    heads = bias_ref.shape[0]
    wide = heads * span
    some_rows = rows // halves
    deep = some_rows // fold
    piece_rows = weights.shape[2]
    part = piece_rows // chunks
    w_cols = w_hbm.shape[1]
    w_rows = w_hbm.shape[0]

    below, above = zone, zones - 1 - zone
    near = jnp.minimum(below, above)
    toward = jnp.where(below <= above, -1, 1)

    def source(n):
        if n == 0:
            return zone
        sign = toward if n % 2 == 1 else -toward
        offset = jnp.where(n <= 2 * near, sign * ((n + 1) // 2), -toward * (n - near))
        return zone + offset

    def at_zone(z):
        return {"sp": z * group + place}

    def at_column(j):
        return {"dp": lax.rem(column + j, columns) * cores + core}

    def at_place(g):
        return {"sp": zone * group + lax.rem(place + g, group)}

    def token_place(g):
        return lax.rem(place - g + group, group)

    partner = {"dp": column * cores + (1 - core)}

    barrier = pltpu.get_barrier_semaphore()
    peers = [
        {"sp": lax.rem(sp + k, size)} for k in range(1, size)
    ] + [at_column(j) for j in range(1, columns)] + [partner]
    for peer in peers:
        pl.semaphore_signal(barrier, inc=1, device_id=peer, device_id_type=MESH)

    wq_copy = pltpu.make_async_copy(wq_hbm, weights.at[zone, 0, pl.ds(0, depth), :], wq_sem)
    wq_copy.start()
    x_copy = pltpu.make_async_copy(x_hbm, x_ref, x_sem)
    x_copy.start()
    own_lanes = pl.ds(pl.multiple_of(dp * w_cols, w_cols), w_cols)
    own_weight = pltpu.make_async_copy(w_hbm, w_all.at[sp, :, own_lanes], own_sem)
    own_weight.start()

    pair = jnp.concatenate([wk_ref[...].astype(f32), wv_ref[...].astype(f32)], axis=0).T
    weights[zone, 0, depth:, :] = jnp.concatenate([pair[:half], pair[half:]], axis=1).astype(bf16)

    below_diag = lax.broadcasted_iota(jnp.int32, (rows, rows), 1) >= lax.broadcasted_iota(
        jnp.int32, (rows, rows), 0
    )
    tri[...] = jnp.where(below_diag, -1.0, 0.0).astype(bf16)
    mark_row = lax.broadcasted_iota(jnp.int32, (aug, wide), 0)
    mark_head = lax.broadcasted_iota(jnp.int32, (aug, wide), 1) // span
    marks = jnp.where(
        (mark_row >= 3 * mark_head) & (mark_row < 3 * mark_head + 3), 1.0, 0.0
    ).astype(bf16)
    for z in range(zones):
        q_t[z, 2 * HEAD_DIM :, :] = marks
    row_of = lax.broadcasted_iota(jnp.int32, (8, span), 0)
    for z in range(zones):
        tokens = slice(z * span, (z + 1) * span)
        terms = jnp.zeros((8, span), f32)
        for h in range(heads):
            value = bias_ref[h : h + 1, tokens] * LOG2E
            high = value.astype(bf16).astype(f32)
            middle = (value - high).astype(bf16).astype(f32)
            low = value - high - middle
            for i, term in enumerate((high, middle, low)):
                terms = jnp.where(row_of == 3 * h + i, term, terms)
        padded = jnp.concatenate([terms, jnp.zeros((120, span), f32)], axis=0)
        k_aug[tokens, 128:256] = padded.T.astype(bf16)

    wq_copy.wait()
    pl.semaphore_wait(barrier, len(peers))

    def piece(z, d):
        return weights.at[z, d]

    def some(z, d, c):
        return weights.at[z, d, pl.ds(c * part, part), :]

    def send_outward(n):
        z = source(n)
        for way, target in ((0, zone - 1), (1, zone + 1)):
            exists = (target >= 0) if way == 0 else (target < zones)
            if n > 0:
                exists = exists & ((z > zone) if way == 0 else (z < zone))
            yield way, at_zone(jnp.clip(target, 0, zones - 1)), exists

    def z_relay(n, c):
        z = source(n)
        for way, peer, exists in send_outward(n):
            copy = remote(some(z, 0, c), some(z, 0, c), send_z.at[n, way], recv_z.at[z, c], peer)

            @pl.when(exists)
            def _(copy=copy):
                copy.start()

    def z_sent(n):
        z = source(n)
        for way, peer, exists in send_outward(n):
            copy = remote(piece(z, 0), piece(z, 0), send_z.at[n, way], recv_z.at[z, 0], peer)

            @pl.when(exists)
            def _(copy=copy):
                copy.wait_send()

    def z_wait(n, c):
        z = source(n)
        remote(
            some(z, 0, c), some(z, 0, c), send_z.at[n, 0], recv_z.at[z, c], at_zone(zone)
        ).wait_recv()

    def x_spread(n, c):
        z = source(n)
        for j in range(1, columns):
            remote(
                some(z, 0, c), some(z, cores * j, c),
                send_x.at[j - 1], recv_x.at[n, j - 1], at_column(j),
            ).start()

    def to_partner(n, j):
        z = source(n)
        remote(
            piece(z, cores * j), piece(z, cores * j + 1), send_c.at[j], recv_c.at[n, j], partner
        ).start()

    def spread_columns(n):
        z = source(n)
        for j in range(1, columns):
            remote(
                piece(z, 0), piece(z, cores * j), send_x.at[j - 1], recv_x.at[n, j - 1], at_column(j)
            ).wait_recv()
            to_partner(n, j)

    def weights_sent():
        for n in range(zones):
            z_sent(n)
        for j in range(1, columns):
            remote(
                weights.at[:, 0], weights.at[:, 0], send_x.at[j - 1], recv_x.at[0, j - 1], partner
            ).wait_send()
        for j in range(columns):
            remote(
                weights.at[:, 0], weights.at[:, 0], send_c.at[j], recv_c.at[0, j], partner
            ).wait_send()

    def arrive(n):
        for c in range(chunks):
            if n > 0:
                z_wait(n, c)
            z_relay(n, c)
            x_spread(n, c)
        to_partner(n, 0)

    def normalize(rows_ref, g, first, count):
        step = 16

        def chunk(i, carry):
            here = pl.ds(pl.multiple_of(first + i * step, step), step)
            full = rows_ref[here, :].astype(f32)
            scale = lax.rsqrt(jnp.mean(full * full, axis=-1, keepdims=True) + norm_eps)
            for d in range(pieces):
                j, c = d // cores, d % cores
                index = lax.rem(column - j + columns, columns) * cores + (
                    core if c == 0 else 1 - core
                )
                for s in range(2):
                    lanes = pl.ds(pl.multiple_of(index * depth + s * half, half), half)
                    some = rows_ref[here, lanes].astype(f32) * scale * in_gain_ref[:, lanes]
                    normed[g, s, here, d * half : (d + 1) * half] = some.astype(bf16)
            return carry

        lax.fori_loop(0, count // step, chunk, 0)

    def project(n, g, parts=tuple(range(halves))):
        z = source(n)
        first, count = parts[0] * some_rows, len(parts) * some_rows
        key_weights = weights[z, :, depth : depth + half, :].reshape(pieces * half, cq)
        both = []
        for s in range(2):
            query_weights = weights[z, :, s * half : (s + 1) * half, :].reshape(pieces * half, cq)
            both.append(
                jnp.dot(
                    normed[g, s, first : first + count, :],
                    jnp.concatenate([query_weights, key_weights], axis=1),
                    preferred_element_type=f32,
                )
            )
        q = (both[0][:, :cq] + both[1][:, :cq]).astype(bf16)
        kv = both[0][:, cq : cq + ck2] + both[1][:, cq + ck2 : cq + 2 * ck2]
        tokens = token_place(g)
        for r in parts:
            mine = slice((r - parts[0]) * some_rows, (r - parts[0] + 1) * some_rows)
            q_part, kv_part = q[mine], kv[mine]
            kv_part = jnp.concatenate(
                [kv_part[i * deep : (i + 1) * deep] for i in range(fold)], axis=1
            ).astype(bf16)
            if n == 0:
                inbox[zone, tokens, r, :some_rows, :] = q_part
                inbox[zone, tokens, r, some_rows:, :] = kv_part
            else:
                outbox[n, g, r, :some_rows, :] = q_part
                outbox[n, g, r, some_rows:, :] = kv_part
        if n > 0:
            sent = pl.ds(parts[0], len(parts))
            remote(
                outbox.at[n, g, sent], inbox.at[zone, tokens, sent],
                send_m, recv_m.at[zone], at_zone(z),
            ).start()

    def share_keys(n):
        z = source(n)
        if n > 0:
            remote(inbox.at[z], inbox.at[z], send_m, recv_m.at[z], at_zone(zone)).wait_recv()
        for i in range(1, group):
            remote(
                inbox.at[z, :, :, pl.ds(some_rows, deep), :], kvbox.at[z, place],
                send_k.at[i - 1], recv_k.at[z, place], at_place(i),
            ).start()
        kvbox[z, place] = inbox[z, :, :, some_rows:, :]

    def keys_sent():
        remote(
            outbox.at[pl.ds(1, zones - 1)], outbox.at[pl.ds(1, zones - 1)],
            send_m, recv_m.at[zone], partner,
        ).wait_send()
        for i in range(1, group):
            every = inbox.at[:, :, :, pl.ds(some_rows, deep), :]
            remote(every, every, send_k.at[i - 1], recv_k.at[zone, place], partner).wait_send()

    def collect(n):
        z = source(n)
        for i in range(1, group):
            owner = token_place(i)
            remote(
                kvbox.at[z, owner], kvbox.at[z, owner],
                send_k.at[i - 1], recv_k.at[z, owner], at_place(i),
            ).wait_recv()
        for t in range(group):
            parts = []
            for p in range(group):
                packed = [kvbox[z, p, t, r].astype(f32) for r in range(halves)]
                parts.append(
                    jnp.concatenate(
                        [
                            packed[r][:, i * ck2 : (i + 1) * ck2]
                            for r in range(halves)
                            for i in range(fold)
                        ],
                        axis=0,
                    )
                )
            keys = [p[:, :ck] for p in parts]
            values = [p[:, ck:] for p in parts]
            target = pl.ds(pl.multiple_of((z * group + t) * rows, rows), rows)
            k_aug[target, 0:128] = jnp.concatenate(keys + keys, axis=1).astype(bf16)
            turned = jnp.concatenate(keys + values, axis=1).T
            v_t[z * group + t] = turned[HEAD_DIM:].astype(bf16)
        q = jnp.concatenate(
            [
                inbox[z, t, r, :some_rows, :].astype(f32)
                for t in range(group)
                for r in range(halves)
            ],
            axis=0,
        )
        turned = q.T * (LOG2E * HEAD_DIM**-0.5)
        high = turned.astype(bf16)
        low = (turned - high.astype(f32)).astype(bf16)
        for h in range(heads):
            lanes = slice(h * span, (h + 1) * span)
            own = slice(h * HEAD_DIM, (h + 1) * HEAD_DIM)
            q_t[z, :HEAD_DIM, lanes] = high[own]
            q_t[z, HEAD_DIM : 2 * HEAD_DIM, lanes] = low[own]

    def attend(qz, kz, diagonal):
        after = None if diagonal else rest[qz]
        acc = None if diagonal else total[qz]
        logits = {}
        for t in reversed(range(group)):
            window = pl.ds(pl.multiple_of((kz * group + t) * rows, rows), rows)
            logits[t] = jnp.dot(
                k_aug[window, : 2 * HEAD_DIM + aug], q_t[qz], preferred_element_type=f32
            )
        for t in reversed(range(group)):
            x = logits[t]
            soft = jnp.maximum(x, lax.log2(1.0 + lax.exp2(jnp.minimum(x, 126.0))))
            if diagonal:
                key = lax.broadcasted_iota(jnp.int32, (rows, wide), 0) + t * rows
                query = lax.rem(lax.broadcasted_iota(jnp.int32, (rows, wide), 1), span)
                strict = key < query
                soft = jnp.where(strict, soft, 0.0)
            kept = jnp.dot(tri[...], soft.astype(bf16), preferred_element_type=f32)
            power = x + kept
            if after is not None:
                power = power + after
            sticks = lax.exp2(power)
            if diagonal:
                sticks = jnp.where(strict, sticks, 0.0)
            more = jnp.dot(v_t[kz * group + t], sticks.astype(bf16), preferred_element_type=f32)
            acc = more if acc is None else acc + more
            after = kept[0:1, :] if after is None else after + kept[0:1, :]
        total[qz] = acc
        rest[qz] = after

    def send_head(s):
        return remote(
            head.at[pl.ds(s * rows, rows), :], arrived.at[sp], send_h, recv_h, {"sp": s}
        )

    def all_heads():
        others = pl.ds(0, (size - 1) * rows)
        return remote(head.at[others, :], head.at[others, :], send_h, recv_h, partner)

    def finish(qz):
        scaled = []
        for h in range(heads):
            some = total[qz, :, h * span : (h + 1) * span]
            scaled.append(
                some * lax.rsqrt(jnp.mean(some * some, axis=0, keepdims=True) + norm_eps)
            )
        lanes = pl.ds(pl.multiple_of(sp * cq, cq), cq) if cq % 128 == 0 else None
        gains = own_gain() if lanes is None else out_gain_ref[:, lanes]
        here = pl.ds(pl.multiple_of(qz * span, span), span)
        head[here, :] = (jnp.concatenate(scaled, axis=0).T * gains).astype(bf16)
        for t in range(group):
            s = qz * group + t

            @pl.when(s != sp)
            def _(s=s):
                send_head(s).start()

    def own_gain():
        both = out_gain_ref[:, pl.ds(pl.multiple_of(sp // 2 * 128, 128), 128)]
        return jnp.where(sp % 2 == 0, both[:, :cq], both[:, cq : 2 * cq])

    balanced = columns == group

    def lean_of(n):
        if not balanced:
            return 0
        return (core, 1, core, 1 - core)[n % 4]

    def weight(n, j, i):
        lean = lean_of(n)
        dx = j * (1 - lean) + i * lean
        dy = j * lean + i * (1 - lean)
        row = source(n) * group + lax.rem(place - dy + group, group)
        lane = lax.rem(column - dx + columns, columns) * cores + core
        return w_all.at[row, :, pl.ds(pl.multiple_of(lane * w_cols, w_cols), w_cols)]

    first_count = columns if not balanced else group
    second_count = group if not balanced else columns

    def at_first(n, j):
        lean = lean_of(n)
        return {
            "sp": zone * group + lax.rem(place + j * lean, group),
            "dp": lax.rem(column + j * (1 - lean), columns) * cores + core,
        }

    def at_second(n, i):
        lean = lean_of(n)
        return {
            "sp": zone * group + lax.rem(place + i * (1 - lean), group),
            "dp": lax.rem(column + i * lean, columns) * cores + core,
        }

    def w_core(n, j, i):
        remote(weight(n, j, i), weight(n, j, i), send_wc, recv_wc, partner).start()

    def w_second(n, j):
        for i in range(1, second_count):
            remote(
                weight(n, j, 0), weight(n, j, 0),
                send_wb.at[i - 1], recv_wb.at[n, j, i - 1], at_second(n, i),
            ).start()
        w_core(n, j, 0)

    def w_first(n):
        for j in range(1, first_count):
            remote(
                weight(n, 0, 0), weight(n, 0, 0),
                send_wa.at[j - 1], recv_wa.at[n, j - 1], at_first(n, j),
            ).start()
        w_second(n, 0)

    def w_sent():
        for n in range(zones):
            z = source(n)
            for way, peer, exists in send_outward(n):
                copy = remote(
                    weight(n, 0, 0), weight(n, 0, 0), send_wz.at[n, way], recv_wz.at[z], peer
                )

                @pl.when(exists)
                def _(copy=copy):
                    copy.wait_send()
        block = w_all.at[pl.ds(0, zones), :, pl.ds(0, w_cols)]
        for j in range(1, first_count):
            remote(block, block, send_wa.at[j - 1], recv_wa.at[0, j - 1], partner).wait_send()
        block = w_all.at[pl.ds(0, zones), :, pl.ds(0, first_count * w_cols)]
        for i in range(1, second_count):
            remote(block, block, send_wb.at[i - 1], recv_wb.at[0, 0, i - 1], partner).wait_send()

    def all_cores():
        block = w_all.at[:, :, pl.ds(0, columns * w_cols)]
        return remote(block, block, send_wc, recv_wc, partner)

    middle_zone = near > 0

    def wz_own(n):
        short = jnp.maximum(2 * near - 1, 0)
        for way, peer, exists in send_outward(0):
            fewer = above < below if way == 0 else below <= above
            last = jnp.where(fewer, short, zones - 1)
            copy = remote(
                weight(0, 0, 0), weight(0, 0, 0), send_wz.at[0, way], recv_wz.at[zone], peer
            )

            @pl.when(exists & (last == n))
            def _(copy=copy):
                copy.start()

    def wz_pass(n, now):
        z = source(n)

        @pl.when(now)
        def _():
            remote(
                weight(n, 0, 0), weight(n, 0, 0), send_wz.at[n, 0], recv_wz.at[z], at_zone(zone)
            ).wait_recv()
            for way, peer, exists in send_outward(n):
                copy = remote(
                    weight(n, 0, 0), weight(n, 0, 0), send_wz.at[n, way], recv_wz.at[z], peer
                )

                @pl.when(exists)
                def _(copy=copy):
                    copy.start()

    def w_first_event(n):
        for j in range(1, first_count):
            remote(
                weight(n, j, 0), weight(n, j, 0),
                send_wa.at[j - 1], recv_wa.at[n, j - 1], at_first(n, j),
            ).wait_recv()
            w_second(n, j)

    def w_second_event(n):
        for j in range(first_count):
            for i in range(1, second_count):
                remote(
                    weight(n, j, i), weight(n, j, i),
                    send_wb.at[i - 1], recv_wb.at[n, j, i - 1], at_second(n, i),
                ).wait_recv()
                w_core(n, j, i)

    def settle(n):
        for j in range(columns):
            z = source(n)
            remote(
                piece(z, cores * j), piece(z, cores * j + 1),
                send_c.at[j], recv_c.at[n, j], partner,
            ).wait_recv()

    def far(g, r):
        first = r * some_rows
        window = pl.ds(first, some_rows)
        return remote(
            x_ref.at[window, :], x_far.at[g - 1, window, :],
            send_y.at[g - 1, r], recv_y.at[g - 1, r], at_place(g),
        )

    def far_arrives(r):
        for g in range(1, group):
            far(g, r).wait_recv()
            normalize(x_far.at[g - 1], g, r * some_rows, some_rows)

    def far_project(n, parts):
        for g in range(1, group):
            project(n, g, parts)

    arrive(0)
    x_copy.wait()
    for r in range(halves):
        for g in range(1, group):
            far(g, r).start()
    own_weight.wait()
    wz_own(0)
    normalize(x_ref, 0, 0, rows)
    end_zone = jnp.logical_not(middle_zone)
    last = zones - 1
    for n in range(1, last):
        arrive(n)
        wz_own(n)
        if n == 1:
            spread_columns(0)
    settle(0)
    project(0, 0)

    @pl.when(middle_zone)
    def _():
        arrive(last)
        wz_own(last)
        wz_pass(1, middle_zone)

    for n in range(1, last):
        if n == last - 1:
            @pl.when(end_zone)
            def _():
                arrive(last)
                wz_own(last)

            w_first(0)
        spread_columns(n)
        if n == 1:
            far_arrives(0)
            far_project(0, (0,))
        settle(n)
        project(n, 0)
        far_project(n, (0,))
    far_arrives(1)
    for n in range(last):
        if n == 1:
            spread_columns(last)
        far_project(n, (1,))
    share_keys(0)
    settle(last)
    for g in range(group):
        project(last, g)
    wz_pass(1, end_zone)

    events = {}

    def at_slot(n, m, event, k):
        n = min(n, zones - 1)
        events.setdefault((n, min(m, n)), []).append((event, k))

    def late(n):
        wz_pass(n, end_zone)
        w_first(n)

    at_slot(1, 0, w_first_event, 1)
    for n in range(2, zones):
        at_slot(n - 1, 2 * n - 4, late, n)
        at_slot(n + 1, 4 * n - 8, w_first_event, n)
    at_slot(2, 0, w_second_event, 0)
    at_slot(2, 2, w_second_event, 1)

    for n in range(zones):
        if n + 1 < zones:
            share_keys(n + 1)
        if n == 0:
            for k in range(2, zones):
                wz_pass(k, middle_zone)
            w_first(1)
            w_first_event(0)
        collect(n)
        a = source(n)
        upward = a > zone if n > 0 else None
        attend(a, a, True)
        if n == 0:
            tiles = [(a, a)]
        else:
            tiles = [(a, a)] + [
                (jnp.where(upward, a, a + m), jnp.where(upward, a - m, a)) for m in range(1, n + 1)
            ]
        for m, (qz, kz) in enumerate(tiles):
            if m > 0:
                attend(qz, kz, False)

            @pl.when(kz == 0)
            def _(qz=qz):
                finish(qz)

            for event, k in events.get((n, m), []):
                event(k)
    for n in range(2, zones):
        w_second_event(n)
    mine = pltpu.make_async_copy(
        head.at[pl.ds(pl.multiple_of(sp * rows, rows), rows), :], arrived.at[sp], own_sem
    )
    mine.start()
    weights_sent()
    keys_sent()
    for r in range(halves):
        for g in range(1, group):
            far(g, r).wait_send()
    w_sent()
    mine.wait()
    all_heads().wait_recv()
    for s in range(size):
        joined[:, s * cq : (s + 1) * cq] = arrived[s]
    all_cores().wait_recv()
    strip = min(512, width)
    for i in range(width // strip):
        lanes = slice(i * strip, (i + 1) * strip)
        out_ref[:, lanes] = jnp.dot(
            joined[...], w_all[:, :, lanes].reshape(size * cq, strip), preferred_element_type=f32
        ).astype(bf16)
    all_cores().wait_send()
    all_heads().wait_send()


def layer(x, in_gain, wq, wk, wv, bias, out_gain, w_out, zones, group):
    rows, width = x.shape
    pieces = lax.axis_size("dp")
    columns = pieces // cores
    size = zones * group
    span = group * rows
    length = size * rows
    depth, cq = wq.shape
    ck2 = 2 * wk.shape[0]
    fold = cq // ck2
    heads = bias.shape[0]
    wide = heads * span
    some_rows = rows // halves
    deep = some_rows // fold
    dma = pltpu.SemaphoreType.DMA
    most = max(columns, group)
    return pl.pallas_call(
        functools.partial(layer_kernel, zones, group),
        out_shape=pltpu.VMEM((rows, width), bf16),
        in_specs=[ANY_SPEC, VMEM_SPEC, ANY_SPEC] + [VMEM_SPEC] * 4 + [ANY_SPEC],
        out_specs=VMEM_SPEC,
        scratch_shapes=[
            pltpu.VMEM((rows, width), bf16),
            pltpu.VMEM((zones, pieces, depth + depth // 2, cq), bf16),
            pltpu.VMEM((group - 1, rows, width), bf16),
            pltpu.VMEM((group, 2, rows, width // 2), bf16),
            pltpu.VMEM((zones, group, halves, some_rows + deep, cq), bf16),
            pltpu.VMEM((zones, group, halves, some_rows + deep, cq), bf16),
            pltpu.VMEM((zones, group, group, halves, deep, cq), bf16),
            pltpu.VMEM((length, 256), bf16),
            pltpu.VMEM((size, HEAD_DIM, rows), bf16),
            pltpu.VMEM((zones, 2 * HEAD_DIM + aug, wide), bf16),
            pltpu.VMEM((zones, 1, wide), f32),
            pltpu.VMEM((zones, HEAD_DIM, wide), f32),
            pltpu.VMEM((rows, rows), bf16),
            pltpu.VMEM((size, w_out.shape[0], width), bf16),
            pltpu.VMEM((length, cq), bf16),
            pltpu.VMEM((size, rows, cq), bf16),
            pltpu.VMEM((rows, size * cq), bf16),
            dma, dma, dma,
            dma((zones, 2)), dma((zones, chunks)),
            dma((columns - 1,)), dma((zones, columns - 1)),
            dma((columns,)), dma((zones, columns)),
            dma((group - 1, halves)), dma((group - 1, halves)),
            dma, dma((zones,)),
            dma((group - 1,)), dma((zones, group)),
            dma((zones, 2)), dma((zones,)),
            dma((most - 1,)), dma((zones, most - 1)),
            dma((most - 1,)), dma((zones, most, most - 1)),
            dma, dma,
            dma, dma,
        ],
        compiler_params=pltpu.CompilerParams(collective_id=0, has_side_effects=True),
        name="layer",
    )(x, in_gain, wq, wk, wv, bias, out_gain, w_out)


def body(inputs, in_gain, w_query, w_key, w_value, key_bias, out_gain, w_out):
    group = HEAD_DIM // w_key.shape[1]
    zones = lax.axis_size("sp") // group
    return layer(
        inputs[0], in_gain[None], w_query, w_key.T, w_value.T, key_bias[0].T,
        out_gain[None], w_out, zones, group,
    )[None]


def solution(mesh):
    placed = (
        P("dp", "sp", None),
        P(),
        P("dp", "sp"),
        P("dp", "sp"),
        P("dp", "sp"),
        P("dp", None, "sp"),
        P(),
        P("sp", "dp"),
    )
    return jax.shard_map(
        body, mesh=mesh, in_specs=placed, out_specs=P("dp", "sp", None), check_vma=False
    )
```

```python
import functools
import math

import jax
import jax.numpy as jnp
from jax import lax
from jax.experimental import pallas as pl
from jax.experimental.pallas import tpu as pltpu
from jax.sharding import PartitionSpec as P

HEAD_DIM = 64
LOG2E = math.log2(math.e)
MESH = pl.DeviceIdType.MESH
VMEM_SPEC = pl.BlockSpec(memory_space=pltpu.VMEM)
ANY_SPEC = pl.BlockSpec(memory_space=pl.ANY)
f32, bf16 = jnp.float32, jnp.bfloat16


norm_eps = 1e-06
cores = 2
chunks = 2
halves = 2
aug = 16


def remote(source, target, send, recv, peer):
    copy = pltpu.make_async_remote_copy(
        src_ref=source, dst_ref=target, send_sem=send, recv_sem=recv,
        device_id=peer, device_id_type=MESH,
    )
    return copy


def layer_kernel(
    zones, group,
    x_hbm, in_gain_ref, wq_hbm, wk_ref, wv_ref, bias_ref, out_gain_ref, w_hbm, out_ref,
    x_ref, weights, x_far, normed, outbox, inbox, kvbox, k_aug, v_t, q_t, rest, total, tri,
    w_all, head, arrived, joined,
    own_sem, x_sem, wq_sem, send_z, recv_z, send_x, recv_x, send_c, recv_c, send_y, recv_y,
    send_m, recv_m, send_k, recv_k,
    send_wz, recv_wz, send_wa, recv_wa, send_wb, recv_wb, send_wc, recv_wc, send_h, recv_h,
):
    columns = lax.axis_size("dp") // cores
    sp, dp = lax.axis_index("sp"), lax.axis_index("dp")
    zone, place = sp // group, sp % group
    column, core = dp // cores, dp % cores
    rows, width = x_ref.shape
    size = zones * group
    span = group * rows
    pieces = columns * cores
    depth = width // pieces
    half = depth // 2
    cq = wq_hbm.shape[1]
    ck = wk_ref.shape[0]
    ck2 = 2 * ck
    fold = cq // ck2
    heads = bias_ref.shape[0]
    wide = heads * span
    some_rows = rows // halves
    deep = some_rows // fold
    piece_rows = weights.shape[2]
    part = piece_rows // chunks
    w_cols = w_hbm.shape[1]
    w_rows = w_hbm.shape[0]

    below, above = zone, zones - 1 - zone
    near = jnp.minimum(below, above)
    toward = jnp.where(below <= above, -1, 1)

    def source(n):
        if n == 0:
            return zone
        sign = toward if n % 2 == 1 else -toward
        offset = jnp.where(n <= 2 * near, sign * ((n + 1) // 2), -toward * (n - near))
        return zone + offset

    def at_zone(z):
        return {"sp": z * group + place}

    def at_column(j):
        return {"dp": lax.rem(column + j, columns) * cores + core}

    def at_place(g):
        return {"sp": zone * group + lax.rem(place + g, group)}

    def token_place(g):
        return lax.rem(place - g + group, group)

    partner = {"dp": column * cores + (1 - core)}

    barrier = pltpu.get_barrier_semaphore()
    peers = [
        {"sp": lax.rem(sp + k, size)} for k in range(1, size)
    ] + [at_column(j) for j in range(1, columns)] + [partner]
    for peer in peers:
        pl.semaphore_signal(barrier, inc=1, device_id=peer, device_id_type=MESH)

    wq_copy = pltpu.make_async_copy(wq_hbm, weights.at[zone, 0, pl.ds(0, depth), :], wq_sem)
    wq_copy.start()
    x_copy = pltpu.make_async_copy(x_hbm, x_ref, x_sem)
    x_copy.start()
    own_lanes = pl.ds(pl.multiple_of(dp * w_cols, w_cols), w_cols)
    own_weight = pltpu.make_async_copy(w_hbm, w_all.at[sp, :, own_lanes], own_sem)
    own_weight.start()

    pair = jnp.concatenate([wk_ref[...].astype(f32), wv_ref[...].astype(f32)], axis=0).T
    weights[zone, 0, depth:, :] = jnp.concatenate([pair[:half], pair[half:]], axis=1).astype(bf16)

    below_diag = lax.broadcasted_iota(jnp.int32, (rows, rows), 1) >= lax.broadcasted_iota(
        jnp.int32, (rows, rows), 0
    )
    tri[...] = jnp.where(below_diag, -1.0, 0.0).astype(bf16)
    mark_row = lax.broadcasted_iota(jnp.int32, (aug, wide), 0)
    mark_head = lax.broadcasted_iota(jnp.int32, (aug, wide), 1) // span
    marks = jnp.where(
        (mark_row >= 3 * mark_head) & (mark_row < 3 * mark_head + 3), 1.0, 0.0
    ).astype(bf16)
    for z in range(zones):
        q_t[z, 2 * HEAD_DIM :, :] = marks
    row_of = lax.broadcasted_iota(jnp.int32, (8, span), 0)
    for z in range(zones):
        tokens = slice(z * span, (z + 1) * span)
        terms = jnp.zeros((8, span), f32)
        for h in range(heads):
            value = bias_ref[h : h + 1, tokens] * LOG2E
            high = value.astype(bf16).astype(f32)
            middle = (value - high).astype(bf16).astype(f32)
            low = value - high - middle
            for i, term in enumerate((high, middle, low)):
                terms = jnp.where(row_of == 3 * h + i, term, terms)
        padded = jnp.concatenate([terms, jnp.zeros((120, span), f32)], axis=0)
        k_aug[tokens, 128:256] = padded.T.astype(bf16)

    wq_copy.wait()
    pl.semaphore_wait(barrier, len(peers))

    def piece(z, d):
        return weights.at[z, d]

    def some(z, d, c):
        return weights.at[z, d, pl.ds(c * part, part), :]

    def send_outward(n):
        z = source(n)
        for way, target in ((0, zone - 1), (1, zone + 1)):
            exists = (target >= 0) if way == 0 else (target < zones)
            if n > 0:
                exists = exists & ((z > zone) if way == 0 else (z < zone))
            yield way, at_zone(jnp.clip(target, 0, zones - 1)), exists

    def z_relay(n, c):
        z = source(n)
        for way, peer, exists in send_outward(n):
            copy = remote(some(z, 0, c), some(z, 0, c), send_z.at[n, way], recv_z.at[z, c], peer)

            @pl.when(exists)
            def _(copy=copy):
                copy.start()

    def z_sent(n):
        z = source(n)
        for way, peer, exists in send_outward(n):
            copy = remote(piece(z, 0), piece(z, 0), send_z.at[n, way], recv_z.at[z, 0], peer)

            @pl.when(exists)
            def _(copy=copy):
                copy.wait_send()

    def z_wait(n, c):
        z = source(n)
        remote(
            some(z, 0, c), some(z, 0, c), send_z.at[n, 0], recv_z.at[z, c], at_zone(zone)
        ).wait_recv()

    def x_spread(n, c):
        z = source(n)
        for j in range(1, columns):
            remote(
                some(z, 0, c), some(z, cores * j, c),
                send_x.at[j - 1], recv_x.at[n, j - 1], at_column(j),
            ).start()

    def to_partner(n, j):
        z = source(n)
        remote(
            piece(z, cores * j), piece(z, cores * j + 1), send_c.at[j], recv_c.at[n, j], partner
        ).start()

    def spread_columns(n):
        z = source(n)
        for j in range(1, columns):
            remote(
                piece(z, 0), piece(z, cores * j), send_x.at[j - 1], recv_x.at[n, j - 1], at_column(j)
            ).wait_recv()
            to_partner(n, j)

    def weights_sent():
        for n in range(zones):
            z_sent(n)
        for j in range(1, columns):
            remote(
                weights.at[:, 0], weights.at[:, 0], send_x.at[j - 1], recv_x.at[0, j - 1], partner
            ).wait_send()
        for j in range(columns):
            remote(
                weights.at[:, 0], weights.at[:, 0], send_c.at[j], recv_c.at[0, j], partner
            ).wait_send()

    def arrive(n):
        for c in range(chunks):
            if n > 0:
                z_wait(n, c)
            z_relay(n, c)
            x_spread(n, c)
        to_partner(n, 0)

    def normalize(rows_ref, g, first, count):
        step = 16

        def chunk(i, carry):
            here = pl.ds(pl.multiple_of(first + i * step, step), step)
            full = rows_ref[here, :].astype(f32)
            scale = lax.rsqrt(jnp.mean(full * full, axis=-1, keepdims=True) + norm_eps)
            for d in range(pieces):
                j, c = d // cores, d % cores
                index = lax.rem(column - j + columns, columns) * cores + (
                    core if c == 0 else 1 - core
                )
                for s in range(2):
                    lanes = pl.ds(pl.multiple_of(index * depth + s * half, half), half)
                    some = rows_ref[here, lanes].astype(f32) * scale * in_gain_ref[:, lanes]
                    normed[g, s, here, d * half : (d + 1) * half] = some.astype(bf16)
            return carry

        lax.fori_loop(0, count // step, chunk, 0)

    def project(n, g, parts=tuple(range(halves))):
        z = source(n)
        first, count = parts[0] * some_rows, len(parts) * some_rows
        key_weights = weights[z, :, depth : depth + half, :].reshape(pieces * half, cq)
        both = []
        for s in range(2):
            query_weights = weights[z, :, s * half : (s + 1) * half, :].reshape(pieces * half, cq)
            both.append(
                jnp.dot(
                    normed[g, s, first : first + count, :],
                    jnp.concatenate([query_weights, key_weights], axis=1),
                    preferred_element_type=f32,
                )
            )
        q = (both[0][:, :cq] + both[1][:, :cq]).astype(bf16)
        kv = both[0][:, cq : cq + ck2] + both[1][:, cq + ck2 : cq + 2 * ck2]
        tokens = token_place(g)
        for r in parts:
            mine = slice((r - parts[0]) * some_rows, (r - parts[0] + 1) * some_rows)
            q_part, kv_part = q[mine], kv[mine]
            kv_part = jnp.concatenate(
                [kv_part[i * deep : (i + 1) * deep] for i in range(fold)], axis=1
            ).astype(bf16)
            if n == 0:
                inbox[zone, tokens, r, :some_rows, :] = q_part
                inbox[zone, tokens, r, some_rows:, :] = kv_part
            else:
                outbox[n, g, r, :some_rows, :] = q_part
                outbox[n, g, r, some_rows:, :] = kv_part
        if n > 0:
            sent = pl.ds(parts[0], len(parts))
            remote(
                outbox.at[n, g, sent], inbox.at[zone, tokens, sent],
                send_m, recv_m.at[zone], at_zone(z),
            ).start()

    def share_keys(n):
        z = source(n)
        if n > 0:
            remote(inbox.at[z], inbox.at[z], send_m, recv_m.at[z], at_zone(zone)).wait_recv()
        for i in range(1, group):
            remote(
                inbox.at[z, :, :, pl.ds(some_rows, deep), :], kvbox.at[z, place],
                send_k.at[i - 1], recv_k.at[z, place], at_place(i),
            ).start()
        kvbox[z, place] = inbox[z, :, :, some_rows:, :]

    def keys_sent():
        remote(
            outbox.at[pl.ds(1, zones - 1)], outbox.at[pl.ds(1, zones - 1)],
            send_m, recv_m.at[zone], partner,
        ).wait_send()
        for i in range(1, group):
            every = inbox.at[:, :, :, pl.ds(some_rows, deep), :]
            remote(every, every, send_k.at[i - 1], recv_k.at[zone, place], partner).wait_send()

    def collect(n):
        z = source(n)
        for i in range(1, group):
            owner = token_place(i)
            remote(
                kvbox.at[z, owner], kvbox.at[z, owner],
                send_k.at[i - 1], recv_k.at[z, owner], at_place(i),
            ).wait_recv()
        for t in range(group):
            parts = []
            for p in range(group):
                packed = [kvbox[z, p, t, r].astype(f32) for r in range(halves)]
                parts.append(
                    jnp.concatenate(
                        [
                            packed[r][:, i * ck2 : (i + 1) * ck2]
                            for r in range(halves)
                            for i in range(fold)
                        ],
                        axis=0,
                    )
                )
            keys = [p[:, :ck] for p in parts]
            values = [p[:, ck:] for p in parts]
            target = pl.ds(pl.multiple_of((z * group + t) * rows, rows), rows)
            k_aug[target, 0:128] = jnp.concatenate(keys + keys, axis=1).astype(bf16)
            turned = jnp.concatenate(keys + values, axis=1).T
            v_t[z * group + t] = turned[HEAD_DIM:].astype(bf16)
        q = jnp.concatenate(
            [
                inbox[z, t, r, :some_rows, :].astype(f32)
                for t in range(group)
                for r in range(halves)
            ],
            axis=0,
        )
        turned = q.T * (LOG2E * HEAD_DIM**-0.5)
        high = turned.astype(bf16)
        low = (turned - high.astype(f32)).astype(bf16)
        for h in range(heads):
            lanes = slice(h * span, (h + 1) * span)
            own = slice(h * HEAD_DIM, (h + 1) * HEAD_DIM)
            q_t[z, :HEAD_DIM, lanes] = high[own]
            q_t[z, HEAD_DIM : 2 * HEAD_DIM, lanes] = low[own]

    def attend(qz, kz, diagonal):
        after = None if diagonal else rest[qz]
        acc = None if diagonal else total[qz]
        logits = {}
        for t in reversed(range(group)):
            window = pl.ds(pl.multiple_of((kz * group + t) * rows, rows), rows)
            logits[t] = jnp.dot(
                k_aug[window, : 2 * HEAD_DIM + aug], q_t[qz], preferred_element_type=f32
            )
        for t in reversed(range(group)):
            x = logits[t]
            soft = jnp.maximum(x, lax.log2(1.0 + lax.exp2(jnp.minimum(x, 126.0))))
            if diagonal:
                key = lax.broadcasted_iota(jnp.int32, (rows, wide), 0) + t * rows
                query = lax.rem(lax.broadcasted_iota(jnp.int32, (rows, wide), 1), span)
                strict = key < query
                soft = jnp.where(strict, soft, 0.0)
            kept = jnp.dot(tri[...], soft.astype(bf16), preferred_element_type=f32)
            power = x + kept
            if after is not None:
                power = power + after
            sticks = lax.exp2(power)
            if diagonal:
                sticks = jnp.where(strict, sticks, 0.0)
            more = jnp.dot(v_t[kz * group + t], sticks.astype(bf16), preferred_element_type=f32)
            acc = more if acc is None else acc + more
            after = kept[0:1, :] if after is None else after + kept[0:1, :]
        total[qz] = acc
        rest[qz] = after

    def send_head(s):
        return remote(
            head.at[pl.ds(s * rows, rows), :], arrived.at[sp], send_h, recv_h, {"sp": s}
        )

    def all_heads():
        others = pl.ds(0, (size - 1) * rows)
        return remote(head.at[others, :], head.at[others, :], send_h, recv_h, partner)

    def finish(qz):
        scaled = []
        for h in range(heads):
            some = total[qz, :, h * span : (h + 1) * span]
            scaled.append(
                some * lax.rsqrt(jnp.mean(some * some, axis=0, keepdims=True) + norm_eps)
            )
        lanes = pl.ds(pl.multiple_of(sp * cq, cq), cq) if cq % 128 == 0 else None
        gains = own_gain() if lanes is None else out_gain_ref[:, lanes]
        here = pl.ds(pl.multiple_of(qz * span, span), span)
        head[here, :] = (jnp.concatenate(scaled, axis=0).T * gains).astype(bf16)
        for t in range(group):
            s = qz * group + t

            @pl.when(s != sp)
            def _(s=s):
                send_head(s).start()

    def own_gain():
        both = out_gain_ref[:, pl.ds(pl.multiple_of(sp // 2 * 128, 128), 128)]
        return jnp.where(sp % 2 == 0, both[:, :cq], both[:, cq : 2 * cq])

    balanced = columns == group

    def lean_of(n):
        if not balanced:
            return 0
        return (core, 1, core, 1 - core)[n % 4]

    def weight(n, j, i):
        lean = lean_of(n)
        dx = j * (1 - lean) + i * lean
        dy = j * lean + i * (1 - lean)
        row = source(n) * group + lax.rem(place - dy + group, group)
        lane = lax.rem(column - dx + columns, columns) * cores + core
        return w_all.at[row, :, pl.ds(pl.multiple_of(lane * w_cols, w_cols), w_cols)]

    first_count = columns if not balanced else group
    second_count = group if not balanced else columns

    def at_first(n, j):
        lean = lean_of(n)
        return {
            "sp": zone * group + lax.rem(place + j * lean, group),
            "dp": lax.rem(column + j * (1 - lean), columns) * cores + core,
        }

    def at_second(n, i):
        lean = lean_of(n)
        return {
            "sp": zone * group + lax.rem(place + i * (1 - lean), group),
            "dp": lax.rem(column + i * lean, columns) * cores + core,
        }

    def w_core(n, j, i):
        remote(weight(n, j, i), weight(n, j, i), send_wc, recv_wc, partner).start()

    def w_second(n, j):
        for i in range(1, second_count):
            remote(
                weight(n, j, 0), weight(n, j, 0),
                send_wb.at[i - 1], recv_wb.at[n, j, i - 1], at_second(n, i),
            ).start()
        w_core(n, j, 0)

    def w_first(n):
        for j in range(1, first_count):
            remote(
                weight(n, 0, 0), weight(n, 0, 0),
                send_wa.at[j - 1], recv_wa.at[n, j - 1], at_first(n, j),
            ).start()
        w_second(n, 0)

    def w_sent():
        for n in range(zones):
            z = source(n)
            for way, peer, exists in send_outward(n):
                copy = remote(
                    weight(n, 0, 0), weight(n, 0, 0), send_wz.at[n, way], recv_wz.at[z], peer
                )

                @pl.when(exists)
                def _(copy=copy):
                    copy.wait_send()
        block = w_all.at[pl.ds(0, zones), :, pl.ds(0, w_cols)]
        for j in range(1, first_count):
            remote(block, block, send_wa.at[j - 1], recv_wa.at[0, j - 1], partner).wait_send()
        block = w_all.at[pl.ds(0, zones), :, pl.ds(0, first_count * w_cols)]
        for i in range(1, second_count):
            remote(block, block, send_wb.at[i - 1], recv_wb.at[0, 0, i - 1], partner).wait_send()

    def all_cores():
        block = w_all.at[:, :, pl.ds(0, columns * w_cols)]
        return remote(block, block, send_wc, recv_wc, partner)

    middle_zone = near > 0

    def wz_own(n):
        short = jnp.maximum(2 * near - 1, 0)
        for way, peer, exists in send_outward(0):
            fewer = above < below if way == 0 else below <= above
            last = jnp.where(fewer, short, zones - 1)
            copy = remote(
                weight(0, 0, 0), weight(0, 0, 0), send_wz.at[0, way], recv_wz.at[zone], peer
            )

            @pl.when(exists & (last == n))
            def _(copy=copy):
                copy.start()

    def wz_pass(n, now):
        z = source(n)

        @pl.when(now)
        def _():
            remote(
                weight(n, 0, 0), weight(n, 0, 0), send_wz.at[n, 0], recv_wz.at[z], at_zone(zone)
            ).wait_recv()
            for way, peer, exists in send_outward(n):
                copy = remote(
                    weight(n, 0, 0), weight(n, 0, 0), send_wz.at[n, way], recv_wz.at[z], peer
                )

                @pl.when(exists)
                def _(copy=copy):
                    copy.start()

    def w_first_event(n):
        for j in range(1, first_count):
            remote(
                weight(n, j, 0), weight(n, j, 0),
                send_wa.at[j - 1], recv_wa.at[n, j - 1], at_first(n, j),
            ).wait_recv()
            w_second(n, j)

    def w_second_event(n):
        for j in range(first_count):
            for i in range(1, second_count):
                remote(
                    weight(n, j, i), weight(n, j, i),
                    send_wb.at[i - 1], recv_wb.at[n, j, i - 1], at_second(n, i),
                ).wait_recv()
                w_core(n, j, i)

    def settle(n):
        for j in range(columns):
            z = source(n)
            remote(
                piece(z, cores * j), piece(z, cores * j + 1),
                send_c.at[j], recv_c.at[n, j], partner,
            ).wait_recv()

    def far(g, r):
        first = r * some_rows
        window = pl.ds(first, some_rows)
        return remote(
            x_ref.at[window, :], x_far.at[g - 1, window, :],
            send_y.at[g - 1, r], recv_y.at[g - 1, r], at_place(g),
        )

    def far_arrives(r):
        for g in range(1, group):
            far(g, r).wait_recv()
            normalize(x_far.at[g - 1], g, r * some_rows, some_rows)

    def far_project(n, parts):
        for g in range(1, group):
            project(n, g, parts)

    arrive(0)
    x_copy.wait()
    for r in range(halves):
        for g in range(1, group):
            far(g, r).start()
    own_weight.wait()
    wz_own(0)
    normalize(x_ref, 0, 0, rows)
    end_zone = jnp.logical_not(middle_zone)
    last = zones - 1
    for n in range(1, last):
        arrive(n)
        wz_own(n)
        if n == 1:
            spread_columns(0)
    settle(0)
    project(0, 0)

    @pl.when(middle_zone)
    def _():
        arrive(last)
        wz_own(last)
        wz_pass(1, middle_zone)

    for n in range(1, last):
        if n == last - 1:
            @pl.when(end_zone)
            def _():
                arrive(last)
                wz_own(last)

        spread_columns(n)
        if n == 1:
            far_arrives(0)
            far_project(0, (0,))
        settle(n)
        project(n, 0)
        far_project(n, (0,))
    far_arrives(1)
    w_first(0)
    for n in range(last):
        if n == 1:
            spread_columns(last)
        far_project(n, (1,))
    share_keys(0)
    settle(last)
    for g in range(group):
        project(last, g)
    wz_pass(1, end_zone)

    events = {}

    def at_slot(n, m, event, k):
        n = min(n, zones - 1)
        events.setdefault((n, min(m, n)), []).append((event, k))

    def late(n):
        wz_pass(n, end_zone)
        w_first(n)

    at_slot(1, 1, w_first_event, 1)
    for k in range(2, min(4, zones)):
        at_slot(1, 1, share_keys, k)
    at_slot(1, 1, late, 2)
    at_slot(2, 1, w_second_event, 0)
    at_slot(2, 2, late, 3)
    at_slot(2, 2, w_second_event, 1)
    at_slot(3, 0, w_first_event, 2)
    at_slot(3, 3, w_first_event, 3)
    at_slot(3, 3, w_second_event, 2)

    for n in range(zones):
        if n == 0:
            wz_pass(2, middle_zone)
            share_keys(1)
            for k in range(3, zones):
                wz_pass(k, middle_zone)
            w_first(1)
            w_first_event(0)
        elif n > 3:
            share_keys(n)
            late(n)
            w_first_event(n)
        collect(n)
        a = source(n)
        upward = a > zone if n > 0 else None
        attend(a, a, True)
        if n == 0:
            tiles = [(a, a)]
        else:
            tiles = [(a, a)] + [
                (jnp.where(upward, a, a + m), jnp.where(upward, a - m, a)) for m in range(1, n + 1)
            ]
        for m, (qz, kz) in enumerate(tiles):
            if m > 0:
                attend(qz, kz, False)

            @pl.when(kz == 0)
            def _(qz=qz):
                finish(qz)

            for event, k in events.get((n, m), []):
                event(k)
    for n in range(3, zones):
        w_second_event(n)
    mine = pltpu.make_async_copy(
        head.at[pl.ds(pl.multiple_of(sp * rows, rows), rows), :], arrived.at[sp], own_sem
    )
    mine.start()
    weights_sent()
    keys_sent()
    for r in range(halves):
        for g in range(1, group):
            far(g, r).wait_send()
    w_sent()
    mine.wait()
    all_heads().wait_recv()
    for s in range(size):
        joined[:, s * cq : (s + 1) * cq] = arrived[s]
    all_cores().wait_recv()
    strip = min(512, width)
    for i in range(width // strip):
        lanes = slice(i * strip, (i + 1) * strip)
        out_ref[:, lanes] = jnp.dot(
            joined[...], w_all[:, :, lanes].reshape(size * cq, strip), preferred_element_type=f32
        ).astype(bf16)
    all_cores().wait_send()
    all_heads().wait_send()


def layer(x, in_gain, wq, wk, wv, bias, out_gain, w_out, zones, group):
    rows, width = x.shape
    pieces = lax.axis_size("dp")
    columns = pieces // cores
    size = zones * group
    span = group * rows
    length = size * rows
    depth, cq = wq.shape
    ck2 = 2 * wk.shape[0]
    fold = cq // ck2
    heads = bias.shape[0]
    wide = heads * span
    some_rows = rows // halves
    deep = some_rows // fold
    dma = pltpu.SemaphoreType.DMA
    most = max(columns, group)
    return pl.pallas_call(
        functools.partial(layer_kernel, zones, group),
        out_shape=pltpu.VMEM((rows, width), bf16),
        in_specs=[ANY_SPEC, VMEM_SPEC, ANY_SPEC] + [VMEM_SPEC] * 4 + [ANY_SPEC],
        out_specs=VMEM_SPEC,
        scratch_shapes=[
            pltpu.VMEM((rows, width), bf16),
            pltpu.VMEM((zones, pieces, depth + depth // 2, cq), bf16),
            pltpu.VMEM((group - 1, rows, width), bf16),
            pltpu.VMEM((group, 2, rows, width // 2), bf16),
            pltpu.VMEM((zones, group, halves, some_rows + deep, cq), bf16),
            pltpu.VMEM((zones, group, halves, some_rows + deep, cq), bf16),
            pltpu.VMEM((zones, group, group, halves, deep, cq), bf16),
            pltpu.VMEM((length, 256), bf16),
            pltpu.VMEM((size, HEAD_DIM, rows), bf16),
            pltpu.VMEM((zones, 2 * HEAD_DIM + aug, wide), bf16),
            pltpu.VMEM((zones, 1, wide), f32),
            pltpu.VMEM((zones, HEAD_DIM, wide), f32),
            pltpu.VMEM((rows, rows), bf16),
            pltpu.VMEM((size, w_out.shape[0], width), bf16),
            pltpu.VMEM((length, cq), bf16),
            pltpu.VMEM((size, rows, cq), bf16),
            pltpu.VMEM((rows, size * cq), bf16),
            dma, dma, dma,
            dma((zones, 2)), dma((zones, chunks)),
            dma((columns - 1,)), dma((zones, columns - 1)),
            dma((columns,)), dma((zones, columns)),
            dma((group - 1, halves)), dma((group - 1, halves)),
            dma, dma((zones,)),
            dma((group - 1,)), dma((zones, group)),
            dma((zones, 2)), dma((zones,)),
            dma((most - 1,)), dma((zones, most - 1)),
            dma((most - 1,)), dma((zones, most, most - 1)),
            dma, dma,
            dma, dma,
        ],
        compiler_params=pltpu.CompilerParams(collective_id=0, has_side_effects=True),
        name="layer",
    )(x, in_gain, wq, wk, wv, bias, out_gain, w_out)


def body(inputs, in_gain, w_query, w_key, w_value, key_bias, out_gain, w_out):
    group = HEAD_DIM // w_key.shape[1]
    zones = lax.axis_size("sp") // group
    return layer(
        inputs[0], in_gain[None], w_query, w_key.T, w_value.T, key_bias[0].T,
        out_gain[None], w_out, zones, group,
    )[None]


def solution(mesh):
    placed = (
        P("dp", "sp", None),
        P(),
        P("dp", "sp"),
        P("dp", "sp"),
        P("dp", "sp"),
        P("dp", None, "sp"),
        P(),
        P("sp", "dp"),
    )
    return jax.shard_map(
        body, mesh=mesh, in_specs=placed, out_specs=P("dp", "sp", None), check_vma=False
    )
```

```python
import functools
import math

import jax
import jax.numpy as jnp
from jax import lax
from jax.experimental import pallas as pl
from jax.experimental.pallas import tpu as pltpu
from jax.sharding import PartitionSpec as P

HEAD_DIM = 64
LOG2E = math.log2(math.e)
MESH = pl.DeviceIdType.MESH
VMEM_SPEC = pl.BlockSpec(memory_space=pltpu.VMEM)
ANY_SPEC = pl.BlockSpec(memory_space=pl.ANY)
f32, bf16 = jnp.float32, jnp.bfloat16


norm_eps = 1e-06
cores = 2
chunks = 2
halves = 2
aug = 16


def remote(source, target, send, recv, peer):
    copy = pltpu.make_async_remote_copy(
        src_ref=source, dst_ref=target, send_sem=send, recv_sem=recv,
        device_id=peer, device_id_type=MESH,
    )
    return copy


def layer_kernel(
    zones, group,
    x_hbm, in_gain_hbm, wq_hbm, wk_hbm, wv_hbm, bias_hbm, out_gain_hbm, w_hbm, out_ref,
    in_gain_ref, wk_ref, wv_ref, bias_ref, out_gain_ref, x_ref, weights, x_far, normed, outbox, inbox, kvbox, k_aug, v_t, q_t, rest, total, tri,
    w_all, head, arrived, joined,
    own_sem, x_sem, wq_sem, small_sem, send_z, recv_z, send_x, recv_x, send_c, recv_c, send_y, recv_y,
    send_m, recv_m, send_k, recv_k,
    send_wz, recv_wz, send_wa, recv_wa, send_wb, recv_wb, send_wc, recv_wc, send_h, recv_h,
):
    columns = lax.axis_size("dp") // cores
    sp, dp = lax.axis_index("sp"), lax.axis_index("dp")
    zone, place = sp // group, sp % group
    column, core = dp // cores, dp % cores
    rows, width = x_ref.shape
    size = zones * group
    span = group * rows
    pieces = columns * cores
    depth = width // pieces
    half = depth // 2
    cq = wq_hbm.shape[1]
    ck = wk_hbm.shape[0]
    ck2 = 2 * ck
    fold = cq // ck2
    heads = bias_hbm.shape[0]
    wide = heads * span
    some_rows = rows // halves
    deep = some_rows // fold
    piece_rows = weights.shape[2]
    part = piece_rows // chunks
    w_cols = w_hbm.shape[1]
    w_rows = w_hbm.shape[0]

    below, above = zone, zones - 1 - zone
    near = jnp.minimum(below, above)
    toward = jnp.where(below <= above, -1, 1)

    def source(n):
        if n == 0:
            return zone
        sign = toward if n % 2 == 1 else -toward
        offset = jnp.where(n <= 2 * near, sign * ((n + 1) // 2), -toward * (n - near))
        return zone + offset

    def at_zone(z):
        return {"sp": z * group + place}

    def at_column(j):
        return {"dp": lax.rem(column + j, columns) * cores + core}

    def at_place(g):
        return {"sp": zone * group + lax.rem(place + g, group)}

    def token_place(g):
        return lax.rem(place - g + group, group)

    partner = {"dp": column * cores + (1 - core)}

    small = [
        pltpu.make_async_copy(source, target, small_sem.at[i])
        for i, (source, target) in enumerate(
            (
                (wk_hbm, wk_ref), (wv_hbm, wv_ref), (bias_hbm, bias_ref),
                (in_gain_hbm, in_gain_ref), (out_gain_hbm, out_gain_ref),
            )
        )
    ]

    barrier = pltpu.get_barrier_semaphore()
    peers = [
        {"sp": lax.rem(sp + k, size)} for k in range(1, size)
    ] + [at_column(j) for j in range(1, columns)] + [partner]
    for peer in peers:
        pl.semaphore_signal(barrier, inc=1, device_id=peer, device_id_type=MESH)

    wq_copy = pltpu.make_async_copy(wq_hbm, weights.at[zone, 0, pl.ds(0, depth), :], wq_sem)
    wq_copy.start()
    x_copy = pltpu.make_async_copy(x_hbm, x_ref, x_sem)
    x_copy.start()
    own_lanes = pl.ds(pl.multiple_of(dp * w_cols, w_cols), w_cols)
    own_weight = pltpu.make_async_copy(w_hbm, w_all.at[sp, :, own_lanes], own_sem)
    for copy in small:
        copy.start()
    own_weight.start()
    for copy in small:
        copy.wait()

    pair = jnp.concatenate([wk_ref[...].astype(f32), wv_ref[...].astype(f32)], axis=0).T
    weights[zone, 0, depth:, :] = jnp.concatenate([pair[:half], pair[half:]], axis=1).astype(bf16)

    below_diag = lax.broadcasted_iota(jnp.int32, (rows, rows), 1) >= lax.broadcasted_iota(
        jnp.int32, (rows, rows), 0
    )
    tri[...] = jnp.where(below_diag, -1.0, 0.0).astype(bf16)
    mark_row = lax.broadcasted_iota(jnp.int32, (aug, wide), 0)
    mark_head = lax.broadcasted_iota(jnp.int32, (aug, wide), 1) // span
    marks = jnp.where(
        (mark_row >= 3 * mark_head) & (mark_row < 3 * mark_head + 3), 1.0, 0.0
    ).astype(bf16)
    for z in range(zones):
        q_t[z, 2 * HEAD_DIM :, :] = marks
    row_of = lax.broadcasted_iota(jnp.int32, (8, span), 0)
    for z in range(zones):
        tokens = slice(z * span, (z + 1) * span)
        terms = jnp.zeros((8, span), f32)
        for h in range(heads):
            value = bias_ref[h : h + 1, tokens] * LOG2E
            high = value.astype(bf16).astype(f32)
            middle = (value - high).astype(bf16).astype(f32)
            low = value - high - middle
            for i, term in enumerate((high, middle, low)):
                terms = jnp.where(row_of == 3 * h + i, term, terms)
        padded = jnp.concatenate([terms, jnp.zeros((120, span), f32)], axis=0)
        k_aug[tokens, 128:256] = padded.T.astype(bf16)

    wq_copy.wait()
    pl.semaphore_wait(barrier, len(peers))

    def piece(z, d):
        return weights.at[z, d]

    def some(z, d, c):
        return weights.at[z, d, pl.ds(c * part, part), :]

    def send_outward(n):
        z = source(n)
        for way, target in ((0, zone - 1), (1, zone + 1)):
            exists = (target >= 0) if way == 0 else (target < zones)
            if n > 0:
                exists = exists & ((z > zone) if way == 0 else (z < zone))
            yield way, at_zone(jnp.clip(target, 0, zones - 1)), exists

    def z_relay(n, c):
        z = source(n)
        for way, peer, exists in send_outward(n):
            copy = remote(some(z, 0, c), some(z, 0, c), send_z.at[n, way], recv_z.at[z, c], peer)

            @pl.when(exists)
            def _(copy=copy):
                copy.start()

    def z_sent(n):
        z = source(n)
        for way, peer, exists in send_outward(n):
            copy = remote(piece(z, 0), piece(z, 0), send_z.at[n, way], recv_z.at[z, 0], peer)

            @pl.when(exists)
            def _(copy=copy):
                copy.wait_send()

    def z_wait(n, c):
        z = source(n)
        remote(
            some(z, 0, c), some(z, 0, c), send_z.at[n, 0], recv_z.at[z, c], at_zone(zone)
        ).wait_recv()

    def x_spread(n, c):
        z = source(n)
        for j in range(1, columns):
            remote(
                some(z, 0, c), some(z, cores * j, c),
                send_x.at[j - 1], recv_x.at[n, j - 1], at_column(j),
            ).start()

    def to_partner(n, j):
        z = source(n)
        remote(
            piece(z, cores * j), piece(z, cores * j + 1), send_c.at[j], recv_c.at[n, j], partner
        ).start()

    def spread_columns(n):
        z = source(n)
        for j in range(1, columns):
            remote(
                piece(z, 0), piece(z, cores * j), send_x.at[j - 1], recv_x.at[n, j - 1], at_column(j)
            ).wait_recv()
            to_partner(n, j)

    def weights_sent():
        for n in range(zones):
            z_sent(n)
        for j in range(1, columns):
            remote(
                weights.at[:, 0], weights.at[:, 0], send_x.at[j - 1], recv_x.at[0, j - 1], partner
            ).wait_send()
        for j in range(columns):
            remote(
                weights.at[:, 0], weights.at[:, 0], send_c.at[j], recv_c.at[0, j], partner
            ).wait_send()

    def arrive(n):
        for c in range(chunks):
            if n > 0:
                z_wait(n, c)
            z_relay(n, c)
            x_spread(n, c)
        to_partner(n, 0)

    def normalize(rows_ref, g, first, count):
        step = 16

        def chunk(i, carry):
            here = pl.ds(pl.multiple_of(first + i * step, step), step)
            full = rows_ref[here, :].astype(f32)
            scale = lax.rsqrt(jnp.mean(full * full, axis=-1, keepdims=True) + norm_eps)
            for d in range(pieces):
                j, c = d // cores, d % cores
                index = lax.rem(column - j + columns, columns) * cores + (
                    core if c == 0 else 1 - core
                )
                for s in range(2):
                    lanes = pl.ds(pl.multiple_of(index * depth + s * half, half), half)
                    some = rows_ref[here, lanes].astype(f32) * scale * in_gain_ref[:, lanes]
                    normed[g, s, here, d * half : (d + 1) * half] = some.astype(bf16)
            return carry

        lax.fori_loop(0, count // step, chunk, 0)

    def project(n, g, parts=tuple(range(halves))):
        z = source(n)
        first, count = parts[0] * some_rows, len(parts) * some_rows
        key_weights = weights[z, :, depth : depth + half, :].reshape(pieces * half, cq)
        both = []
        for s in range(2):
            query_weights = weights[z, :, s * half : (s + 1) * half, :].reshape(pieces * half, cq)
            both.append(
                jnp.dot(
                    normed[g, s, first : first + count, :],
                    jnp.concatenate([query_weights, key_weights], axis=1),
                    preferred_element_type=f32,
                )
            )
        q = (both[0][:, :cq] + both[1][:, :cq]).astype(bf16)
        kv = both[0][:, cq : cq + ck2] + both[1][:, cq + ck2 : cq + 2 * ck2]
        tokens = token_place(g)
        for r in parts:
            mine = slice((r - parts[0]) * some_rows, (r - parts[0] + 1) * some_rows)
            q_part, kv_part = q[mine], kv[mine]
            kv_part = jnp.concatenate(
                [kv_part[i * deep : (i + 1) * deep] for i in range(fold)], axis=1
            ).astype(bf16)
            if n == 0:
                inbox[zone, tokens, r, :some_rows, :] = q_part
                inbox[zone, tokens, r, some_rows:, :] = kv_part
            else:
                outbox[n, g, r, :some_rows, :] = q_part
                outbox[n, g, r, some_rows:, :] = kv_part
        if n > 0:
            sent = pl.ds(parts[0], len(parts))
            remote(
                outbox.at[n, g, sent], inbox.at[zone, tokens, sent],
                send_m, recv_m.at[zone], at_zone(z),
            ).start()

    def share_keys(n):
        z = source(n)
        if n > 0:
            remote(inbox.at[z], inbox.at[z], send_m, recv_m.at[z], at_zone(zone)).wait_recv()
        for i in range(1, group):
            remote(
                inbox.at[z, :, :, pl.ds(some_rows, deep), :], kvbox.at[z, place],
                send_k.at[i - 1], recv_k.at[z, place], at_place(i),
            ).start()
        kvbox[z, place] = inbox[z, :, :, some_rows:, :]

    def keys_sent():
        remote(
            outbox.at[pl.ds(1, zones - 1)], outbox.at[pl.ds(1, zones - 1)],
            send_m, recv_m.at[zone], partner,
        ).wait_send()
        for i in range(1, group):
            every = inbox.at[:, :, :, pl.ds(some_rows, deep), :]
            remote(every, every, send_k.at[i - 1], recv_k.at[zone, place], partner).wait_send()

    def collect(n):
        z = source(n)
        q = jnp.concatenate(
            [
                inbox[z, t, r, :some_rows, :].astype(f32)
                for t in range(group)
                for r in range(halves)
            ],
            axis=0,
        )
        turned = q.T * (LOG2E * HEAD_DIM**-0.5)
        high = turned.astype(bf16)
        low = (turned - high.astype(f32)).astype(bf16)
        for h in range(heads):
            lanes = slice(h * span, (h + 1) * span)
            own = slice(h * HEAD_DIM, (h + 1) * HEAD_DIM)
            q_t[z, :HEAD_DIM, lanes] = high[own]
            q_t[z, HEAD_DIM : 2 * HEAD_DIM, lanes] = low[own]
        for i in range(1, group):
            owner = token_place(i)
            remote(
                kvbox.at[z, owner], kvbox.at[z, owner],
                send_k.at[i - 1], recv_k.at[z, owner], at_place(i),
            ).wait_recv()
        for t in range(group):
            parts = []
            for p in range(group):
                packed = [kvbox[z, p, t, r].astype(f32) for r in range(halves)]
                parts.append(
                    jnp.concatenate(
                        [
                            packed[r][:, i * ck2 : (i + 1) * ck2]
                            for r in range(halves)
                            for i in range(fold)
                        ],
                        axis=0,
                    )
                )
            keys = [p[:, :ck] for p in parts]
            values = [p[:, ck:] for p in parts]
            target = pl.ds(pl.multiple_of((z * group + t) * rows, rows), rows)
            k_aug[target, 0:128] = jnp.concatenate(keys + keys, axis=1).astype(bf16)
            turned = jnp.concatenate(keys + values, axis=1).T
            v_t[z * group + t] = turned[HEAD_DIM:].astype(bf16)

    def attend(qz, kz, diagonal):
        after = None if diagonal else rest[qz]
        acc = None if diagonal else total[qz]
        logits = {}
        for t in reversed(range(group)):
            window = pl.ds(pl.multiple_of((kz * group + t) * rows, rows), rows)
            logits[t] = jnp.dot(
                k_aug[window, : 2 * HEAD_DIM + aug], q_t[qz], preferred_element_type=f32
            )
        for t in reversed(range(group)):
            x = logits[t]
            soft = jnp.maximum(x, lax.log2(1.0 + lax.exp2(jnp.minimum(x, 126.0))))
            if diagonal:
                key = lax.broadcasted_iota(jnp.int32, (rows, wide), 0) + t * rows
                query = lax.rem(lax.broadcasted_iota(jnp.int32, (rows, wide), 1), span)
                strict = key < query
                soft = jnp.where(strict, soft, 0.0)
            kept = jnp.dot(tri[...], soft.astype(bf16), preferred_element_type=f32)
            power = x + kept
            if after is not None:
                power = power + after
            sticks = lax.exp2(power)
            if diagonal:
                sticks = jnp.where(strict, sticks, 0.0)
            more = jnp.dot(v_t[kz * group + t], sticks.astype(bf16), preferred_element_type=f32)
            acc = more if acc is None else acc + more
            after = kept[0:1, :] if after is None else after + kept[0:1, :]
        total[qz] = acc
        rest[qz] = after

    def send_head(s):
        return remote(
            head.at[pl.ds(s * rows, rows), :], arrived.at[sp], send_h, recv_h, {"sp": s}
        )

    def all_heads():
        others = pl.ds(0, (size - 1) * rows)
        return remote(head.at[others, :], head.at[others, :], send_h, recv_h, partner)

    def finish(qz):
        scaled = []
        for h in range(heads):
            some = total[qz, :, h * span : (h + 1) * span]
            scaled.append(
                some * lax.rsqrt(jnp.mean(some * some, axis=0, keepdims=True) + norm_eps)
            )
        lanes = pl.ds(pl.multiple_of(sp * cq, cq), cq) if cq % 128 == 0 else None
        gains = own_gain() if lanes is None else out_gain_ref[:, lanes]
        here = pl.ds(pl.multiple_of(qz * span, span), span)
        head[here, :] = (jnp.concatenate(scaled, axis=0).T * gains).astype(bf16)
        for t in range(group):
            s = qz * group + t

            @pl.when(s != sp)
            def _(s=s):
                send_head(s).start()

    def own_gain():
        both = out_gain_ref[:, pl.ds(pl.multiple_of(sp // 2 * 128, 128), 128)]
        return jnp.where(sp % 2 == 0, both[:, :cq], both[:, cq : 2 * cq])

    balanced = columns == group

    def lean_of(n):
        if not balanced:
            return 0
        return (core, 1, core, 1 - core)[n % 4]

    def weight(n, j, i):
        lean = lean_of(n)
        dx = j * (1 - lean) + i * lean
        dy = j * lean + i * (1 - lean)
        row = source(n) * group + lax.rem(place - dy + group, group)
        lane = lax.rem(column - dx + columns, columns) * cores + core
        return w_all.at[row, :, pl.ds(pl.multiple_of(lane * w_cols, w_cols), w_cols)]

    first_count = columns if not balanced else group
    second_count = group if not balanced else columns

    def at_first(n, j):
        lean = lean_of(n)
        return {
            "sp": zone * group + lax.rem(place + j * lean, group),
            "dp": lax.rem(column + j * (1 - lean), columns) * cores + core,
        }

    def at_second(n, i):
        lean = lean_of(n)
        return {
            "sp": zone * group + lax.rem(place + i * (1 - lean), group),
            "dp": lax.rem(column + i * lean, columns) * cores + core,
        }

    def w_core(n, j, i):
        remote(weight(n, j, i), weight(n, j, i), send_wc, recv_wc, partner).start()

    def w_second(n, j):
        for i in range(1, second_count):
            remote(
                weight(n, j, 0), weight(n, j, 0),
                send_wb.at[i - 1], recv_wb.at[n, j, i - 1], at_second(n, i),
            ).start()
        w_core(n, j, 0)

    def w_first(n):
        for j in range(1, first_count):
            remote(
                weight(n, 0, 0), weight(n, 0, 0),
                send_wa.at[j - 1], recv_wa.at[n, j - 1], at_first(n, j),
            ).start()
        w_second(n, 0)

    def w_sent():
        for n in range(zones):
            z = source(n)
            for way, peer, exists in send_outward(n):
                copy = remote(
                    weight(n, 0, 0), weight(n, 0, 0), send_wz.at[n, way], recv_wz.at[z], peer
                )

                @pl.when(exists)
                def _(copy=copy):
                    copy.wait_send()
        block = w_all.at[pl.ds(0, zones), :, pl.ds(0, w_cols)]
        for j in range(1, first_count):
            remote(block, block, send_wa.at[j - 1], recv_wa.at[0, j - 1], partner).wait_send()
        block = w_all.at[pl.ds(0, zones), :, pl.ds(0, first_count * w_cols)]
        for i in range(1, second_count):
            remote(block, block, send_wb.at[i - 1], recv_wb.at[0, 0, i - 1], partner).wait_send()

    def all_cores():
        block = w_all.at[:, :, pl.ds(0, columns * w_cols)]
        return remote(block, block, send_wc, recv_wc, partner)

    middle_zone = near > 0

    def wz_own(n):
        short = jnp.maximum(2 * near - 1, 0)
        for way, peer, exists in send_outward(0):
            fewer = above < below if way == 0 else below <= above
            last = jnp.where(fewer, short, zones - 1)
            copy = remote(
                weight(0, 0, 0), weight(0, 0, 0), send_wz.at[0, way], recv_wz.at[zone], peer
            )

            @pl.when(exists & (last == n))
            def _(copy=copy):
                copy.start()

    def wz_pass(n, now):
        z = source(n)

        @pl.when(now)
        def _():
            remote(
                weight(n, 0, 0), weight(n, 0, 0), send_wz.at[n, 0], recv_wz.at[z], at_zone(zone)
            ).wait_recv()
            for way, peer, exists in send_outward(n):
                copy = remote(
                    weight(n, 0, 0), weight(n, 0, 0), send_wz.at[n, way], recv_wz.at[z], peer
                )

                @pl.when(exists)
                def _(copy=copy):
                    copy.start()

    def w_first_event(n):
        for j in range(1, first_count):
            remote(
                weight(n, j, 0), weight(n, j, 0),
                send_wa.at[j - 1], recv_wa.at[n, j - 1], at_first(n, j),
            ).wait_recv()
            w_second(n, j)

    def w_second_event(n):
        for j in range(first_count):
            for i in range(1, second_count):
                remote(
                    weight(n, j, i), weight(n, j, i),
                    send_wb.at[i - 1], recv_wb.at[n, j, i - 1], at_second(n, i),
                ).wait_recv()
                w_core(n, j, i)

    def settle(n):
        for j in range(columns):
            z = source(n)
            remote(
                piece(z, cores * j), piece(z, cores * j + 1),
                send_c.at[j], recv_c.at[n, j], partner,
            ).wait_recv()

    def far(g, r):
        first = r * some_rows
        window = pl.ds(first, some_rows)
        return remote(
            x_ref.at[window, :], x_far.at[g - 1, window, :],
            send_y.at[g - 1, r], recv_y.at[g - 1, r], at_place(g),
        )

    def far_arrives(r):
        for g in range(1, group):
            far(g, r).wait_recv()
            normalize(x_far.at[g - 1], g, r * some_rows, some_rows)

    def far_project(n, parts):
        for g in range(1, group):
            project(n, g, parts)

    arrive(0)
    x_copy.wait()
    for r in range(halves):
        for g in range(1, group):
            far(g, r).start()
    own_weight.wait()
    wz_own(0)
    normalize(x_ref, 0, 0, rows)
    end_zone = jnp.logical_not(middle_zone)
    last = zones - 1
    def late(n):
        wz_pass(n, end_zone)
        w_first(n)

    def pass_on(n):
        wz_pass(n, middle_zone)

    plan = {
        "far": [(w_first, 0)],
        (1, 1): [(w_first_event, 1), (share_keys, 2), (share_keys, 3), (late, 2)],
        "projected": [(pass_on, 2)],
        "start": [(pass_on, 3), (late, 1), (w_first_event, 0)],
        (2, 1): [(w_second_event, 0)],
        (2, 2): [(late, 3), (w_second_event, 1), (w_first_event, 2)],
        (3, 3): [(w_first_event, 3), (w_second_event, 2)],
    }

    def run(slot):
        for event, k in plan.get(slot, ()):
            event(k)

    for n in range(1, last):
        arrive(n)
        wz_own(n)
        if n == 1:
            spread_columns(0)
    settle(0)
    project(0, 0)

    @pl.when(middle_zone)
    def _():
        arrive(last)
        wz_own(last)
        wz_pass(1, middle_zone)

    for n in range(1, last):
        if n == last - 1:
            @pl.when(end_zone)
            def _():
                arrive(last)
                wz_own(last)

        spread_columns(n)
        if n == 1:
            far_arrives(0)
            far_project(0, (0,))
        settle(n)
        project(n, 0)
        far_project(n, (0,))
        run(("early", n))
    far_arrives(1)
    run("far")
    for n in range(last):
        if n == 1:
            spread_columns(last)
        far_project(n, (1,))
    share_keys(0)
    run("shared")
    settle(last)
    for g in range(group):
        project(last, g)
    run("projected")

    for n in range(zones):
        if n == 0:
            share_keys(1)
            run("start")
        elif n > 3:
            share_keys(n)
            late(n)
            w_first_event(n)
        collect(n)
        a = source(n)
        upward = a > zone if n > 0 else None
        attend(a, a, True)
        if n == 0:
            tiles = [(a, a)]
        else:
            tiles = [(a, a)] + [
                (jnp.where(upward, a, a + m), jnp.where(upward, a - m, a)) for m in range(1, n + 1)
            ]
        for m, (qz, kz) in enumerate(tiles):
            if m > 0:
                attend(qz, kz, False)

            @pl.when(kz == 0)
            def _(qz=qz):
                finish(qz)

            run((n, m))
    for n in range(3, zones):
        w_second_event(n)
    mine = pltpu.make_async_copy(
        head.at[pl.ds(pl.multiple_of(sp * rows, rows), rows), :], arrived.at[sp], own_sem
    )
    mine.start()
    weights_sent()
    keys_sent()
    for r in range(halves):
        for g in range(1, group):
            far(g, r).wait_send()
    w_sent()
    mine.wait()
    all_heads().wait_recv()
    for s in range(size):
        joined[:, s * cq : (s + 1) * cq] = arrived[s]
    def multiply(c):
        for j in range(columns):
            lanes = pl.ds(pl.multiple_of((j * cores + c) * w_cols, w_cols), w_cols)
            out_ref[:, lanes] = jnp.dot(
                joined[...], w_all[:, :, lanes].reshape(size * cq, w_cols),
                preferred_element_type=f32,
            ).astype(bf16)

    multiply(core)
    all_cores().wait_recv()
    multiply(1 - core)
    all_cores().wait_send()
    all_heads().wait_send()


def layer(x, in_gain, wq, wk, wv, bias, out_gain, w_out, zones, group):
    rows, width = x.shape
    pieces = lax.axis_size("dp")
    columns = pieces // cores
    size = zones * group
    span = group * rows
    length = size * rows
    depth, cq = wq.shape
    ck2 = 2 * wk.shape[0]
    fold = cq // ck2
    heads = bias.shape[0]
    wide = heads * span
    some_rows = rows // halves
    deep = some_rows // fold
    dma = pltpu.SemaphoreType.DMA
    most = max(columns, group)
    return pl.pallas_call(
        functools.partial(layer_kernel, zones, group),
        out_shape=pltpu.VMEM((rows, width), bf16),
        in_specs=[ANY_SPEC] * 8,
        out_specs=VMEM_SPEC,
        scratch_shapes=[
            pltpu.VMEM(in_gain.shape, f32),
            pltpu.VMEM(wk.shape, bf16),
            pltpu.VMEM(wv.shape, bf16),
            pltpu.VMEM(bias.shape, f32),
            pltpu.VMEM(out_gain.shape, f32),
            pltpu.VMEM((rows, width), bf16),
            pltpu.VMEM((zones, pieces, depth + depth // 2, cq), bf16),
            pltpu.VMEM((group - 1, rows, width), bf16),
            pltpu.VMEM((group, 2, rows, width // 2), bf16),
            pltpu.VMEM((zones, group, halves, some_rows + deep, cq), bf16),
            pltpu.VMEM((zones, group, halves, some_rows + deep, cq), bf16),
            pltpu.VMEM((zones, group, group, halves, deep, cq), bf16),
            pltpu.VMEM((length, 256), bf16),
            pltpu.VMEM((size, HEAD_DIM, rows), bf16),
            pltpu.VMEM((zones, 2 * HEAD_DIM + aug, wide), bf16),
            pltpu.VMEM((zones, 1, wide), f32),
            pltpu.VMEM((zones, HEAD_DIM, wide), f32),
            pltpu.VMEM((rows, rows), bf16),
            pltpu.VMEM((size, w_out.shape[0], width), bf16),
            pltpu.VMEM((length, cq), bf16),
            pltpu.VMEM((size, rows, cq), bf16),
            pltpu.VMEM((rows, size * cq), bf16),
            dma, dma, dma, dma((5,)),
            dma((zones, 2)), dma((zones, chunks)),
            dma((columns - 1,)), dma((zones, columns - 1)),
            dma((columns,)), dma((zones, columns)),
            dma((group - 1, halves)), dma((group - 1, halves)),
            dma, dma((zones,)),
            dma((group - 1,)), dma((zones, group)),
            dma((zones, 2)), dma((zones,)),
            dma((most - 1,)), dma((zones, most - 1)),
            dma((most - 1,)), dma((zones, most, most - 1)),
            dma, dma,
            dma, dma,
        ],
        compiler_params=pltpu.CompilerParams(collective_id=0, has_side_effects=True),
        name="layer",
    )(x, in_gain, wq, wk, wv, bias, out_gain, w_out)


def body(inputs, in_gain, w_query, w_key, w_value, key_bias, out_gain, w_out):
    group = HEAD_DIM // w_key.shape[1]
    zones = lax.axis_size("sp") // group
    return layer(
        inputs[0], in_gain[None], w_query, w_key.T, w_value.T, key_bias[0].T,
        out_gain[None], w_out, zones, group,
    )[None]


def solution(mesh):
    placed = (
        P("dp", "sp", None),
        P(),
        P("dp", "sp"),
        P("dp", "sp"),
        P("dp", "sp"),
        P("dp", None, "sp"),
        P(),
        P("sp", "dp"),
    )
    return jax.shard_map(
        body, mesh=mesh, in_specs=placed, out_specs=P("dp", "sp", None), check_vma=False
    )
```

```python
import functools
import math

import jax
import jax.numpy as jnp
from jax import lax
from jax.experimental import pallas as pl
from jax.experimental.pallas import tpu as pltpu
from jax.sharding import PartitionSpec as P

HEAD_DIM = 64
LOG2E = math.log2(math.e)
MESH = pl.DeviceIdType.MESH
VMEM_SPEC = pl.BlockSpec(memory_space=pltpu.VMEM)
ANY_SPEC = pl.BlockSpec(memory_space=pl.ANY)
f32, bf16 = jnp.float32, jnp.bfloat16


norm_eps = 1e-06
cores = 2
chunks = 2
halves = 2
aug = 16


def remote(source, target, send, recv, peer):
    copy = pltpu.make_async_remote_copy(
        src_ref=source, dst_ref=target, send_sem=send, recv_sem=recv,
        device_id=peer, device_id_type=MESH,
    )
    return copy


def layer_kernel(
    zones, group,
    x_hbm, in_gain_hbm, wq_hbm, wk_hbm, wv_hbm, bias_hbm, out_gain_hbm, w_hbm, out_ref,
    in_gain_ref, wk_ref, wv_ref, bias_ref, out_gain_ref, x_ref, weights, x_far, normed, outbox, inbox, kvbox, k_aug, v_t, q_t, rest, total, tri,
    w_all, head, arrived, joined,
    own_sem, x_sem, wq_sem, small_sem, send_z, recv_z, send_x, recv_x, send_c, recv_c, send_y, recv_y,
    send_m, recv_m, send_k, recv_k,
    send_wz, recv_wz, send_wa, recv_wa, send_wb, recv_wb, send_wc, recv_wc, send_h, recv_h,
):
    columns = lax.axis_size("dp") // cores
    sp, dp = lax.axis_index("sp"), lax.axis_index("dp")
    zone, place = sp // group, sp % group
    column, core = dp // cores, dp % cores
    rows, width = x_ref.shape
    size = zones * group
    span = group * rows
    pieces = columns * cores
    depth = width // pieces
    half = depth // 2
    cq = wq_hbm.shape[1]
    ck = wk_hbm.shape[0]
    ck2 = 2 * ck
    fold = cq // ck2
    heads = bias_hbm.shape[0]
    wide = heads * span
    some_rows = rows // halves
    deep = some_rows // fold
    piece_rows = weights.shape[2]
    part = piece_rows // chunks
    w_cols = w_hbm.shape[1]
    w_rows = w_hbm.shape[0]

    below, above = zone, zones - 1 - zone
    near = jnp.minimum(below, above)
    toward = jnp.where(below <= above, -1, 1)

    def source(n):
        if n == 0:
            return zone
        sign = toward if n % 2 == 1 else -toward
        offset = jnp.where(n <= 2 * near, sign * ((n + 1) // 2), -toward * (n - near))
        return zone + offset

    def at_zone(z):
        return {"sp": z * group + place}

    def at_column(j):
        return {"dp": lax.rem(column + j, columns) * cores + core}

    def at_place(g):
        return {"sp": zone * group + lax.rem(place + g, group)}

    def token_place(g):
        return lax.rem(place - g + group, group)

    partner = {"dp": column * cores + (1 - core)}

    small = [
        pltpu.make_async_copy(source, target, small_sem.at[i])
        for i, (source, target) in enumerate(
            (
                (wk_hbm, wk_ref), (wv_hbm, wv_ref), (bias_hbm, bias_ref),
                (in_gain_hbm, in_gain_ref), (out_gain_hbm, out_gain_ref),
            )
        )
    ]

    barrier = pltpu.get_barrier_semaphore()
    peers = [
        {"sp": lax.rem(sp + k, size)} for k in range(1, size)
    ] + [at_column(j) for j in range(1, columns)] + [partner]
    for peer in peers:
        pl.semaphore_signal(barrier, inc=1, device_id=peer, device_id_type=MESH)

    wq_copy = pltpu.make_async_copy(wq_hbm, weights.at[zone, 0, pl.ds(0, depth), :], wq_sem)
    wq_copy.start()
    x_copy = pltpu.make_async_copy(x_hbm, x_ref, x_sem)
    x_copy.start()
    own_lanes = pl.ds(pl.multiple_of(dp * w_cols, w_cols), w_cols)
    own_weight = pltpu.make_async_copy(w_hbm, w_all.at[sp, :, own_lanes], own_sem)
    for copy in small:
        copy.start()
    own_weight.start()
    for copy in small:
        copy.wait()

    pair = jnp.concatenate([wk_ref[...].astype(f32), wv_ref[...].astype(f32)], axis=0).T
    weights[zone, 0, depth:, :] = jnp.concatenate([pair[:half], pair[half:]], axis=1).astype(bf16)

    below_diag = lax.broadcasted_iota(jnp.int32, (rows, rows), 1) >= lax.broadcasted_iota(
        jnp.int32, (rows, rows), 0
    )
    tri[...] = jnp.where(below_diag, -1.0, 0.0).astype(bf16)
    mark_row = lax.broadcasted_iota(jnp.int32, (aug, wide), 0)
    mark_head = lax.broadcasted_iota(jnp.int32, (aug, wide), 1) // span
    marks = jnp.where(
        (mark_row >= 3 * mark_head) & (mark_row < 3 * mark_head + 3), 1.0, 0.0
    ).astype(bf16)
    for z in range(zones):
        q_t[z, 2 * HEAD_DIM :, :] = marks
    row_of = lax.broadcasted_iota(jnp.int32, (8, span), 0)
    for z in range(zones):
        tokens = slice(z * span, (z + 1) * span)
        terms = jnp.zeros((8, span), f32)
        for h in range(heads):
            value = bias_ref[h : h + 1, tokens] * LOG2E
            high = value.astype(bf16).astype(f32)
            middle = (value - high).astype(bf16).astype(f32)
            low = value - high - middle
            for i, term in enumerate((high, middle, low)):
                terms = jnp.where(row_of == 3 * h + i, term, terms)
        padded = jnp.concatenate([terms, jnp.zeros((120, span), f32)], axis=0)
        k_aug[tokens, 128:256] = padded.T.astype(bf16)

    wq_copy.wait()
    pl.semaphore_wait(barrier, len(peers))

    def piece(z, d):
        return weights.at[z, d]

    def some(z, d, c):
        return weights.at[z, d, pl.ds(c * part, part), :]

    def send_outward(n):
        z = source(n)
        for way, target in ((0, zone - 1), (1, zone + 1)):
            exists = (target >= 0) if way == 0 else (target < zones)
            if n > 0:
                exists = exists & ((z > zone) if way == 0 else (z < zone))
            yield way, at_zone(jnp.clip(target, 0, zones - 1)), exists

    def z_relay(n, c):
        z = source(n)
        for way, peer, exists in send_outward(n):
            copy = remote(some(z, 0, c), some(z, 0, c), send_z.at[n, way], recv_z.at[z, c], peer)

            @pl.when(exists)
            def _(copy=copy):
                copy.start()

    def z_sent(n):
        z = source(n)
        for way, peer, exists in send_outward(n):
            copy = remote(piece(z, 0), piece(z, 0), send_z.at[n, way], recv_z.at[z, 0], peer)

            @pl.when(exists)
            def _(copy=copy):
                copy.wait_send()

    def z_wait(n, c):
        z = source(n)
        remote(
            some(z, 0, c), some(z, 0, c), send_z.at[n, 0], recv_z.at[z, c], at_zone(zone)
        ).wait_recv()

    def x_spread(n, c):
        z = source(n)
        for j in range(1, columns):
            remote(
                some(z, 0, c), some(z, cores * j, c),
                send_x.at[j - 1], recv_x.at[n, j - 1], at_column(j),
            ).start()

    def to_partner(n, j):
        z = source(n)
        remote(
            piece(z, cores * j), piece(z, cores * j + 1), send_c.at[j], recv_c.at[n, j], partner
        ).start()

    def spread_columns(n):
        z = source(n)
        for j in range(1, columns):
            remote(
                piece(z, 0), piece(z, cores * j), send_x.at[j - 1], recv_x.at[n, j - 1], at_column(j)
            ).wait_recv()
            to_partner(n, j)

    def weights_sent():
        for n in range(zones):
            z_sent(n)
        for j in range(1, columns):
            remote(
                weights.at[:, 0], weights.at[:, 0], send_x.at[j - 1], recv_x.at[0, j - 1], partner
            ).wait_send()
        for j in range(columns):
            remote(
                weights.at[:, 0], weights.at[:, 0], send_c.at[j], recv_c.at[0, j], partner
            ).wait_send()

    def arrive(n):
        for c in range(chunks):
            if n > 0:
                z_wait(n, c)
            z_relay(n, c)
            x_spread(n, c)
        to_partner(n, 0)

    def normalize(rows_ref, g, first, count):
        step = 16

        def chunk(i, carry):
            here = pl.ds(pl.multiple_of(first + i * step, step), step)
            full = rows_ref[here, :].astype(f32)
            scale = lax.rsqrt(jnp.mean(full * full, axis=-1, keepdims=True) + norm_eps)
            for d in range(pieces):
                j, c = d // cores, d % cores
                index = lax.rem(column - j + columns, columns) * cores + (
                    core if c == 0 else 1 - core
                )
                for s in range(2):
                    lanes = pl.ds(pl.multiple_of(index * depth + s * half, half), half)
                    some = rows_ref[here, lanes].astype(f32) * scale * in_gain_ref[:, lanes]
                    normed[g, s, here, d * half : (d + 1) * half] = some.astype(bf16)
            return carry

        lax.fori_loop(0, count // step, chunk, 0)

    def project(n, g, parts=tuple(range(halves))):
        z = source(n)
        first, count = parts[0] * some_rows, len(parts) * some_rows
        key_weights = weights[z, :, depth : depth + half, :].reshape(pieces * half, cq)
        both = []
        for s in range(2):
            query_weights = weights[z, :, s * half : (s + 1) * half, :].reshape(pieces * half, cq)
            both.append(
                jnp.dot(
                    normed[g, s, first : first + count, :],
                    jnp.concatenate([query_weights, key_weights], axis=1),
                    preferred_element_type=f32,
                )
            )
        q = (both[0][:, :cq] + both[1][:, :cq]).astype(bf16)
        kv = both[0][:, cq : cq + ck2] + both[1][:, cq + ck2 : cq + 2 * ck2]
        tokens = token_place(g)
        for r in parts:
            mine = slice((r - parts[0]) * some_rows, (r - parts[0] + 1) * some_rows)
            q_part, kv_part = q[mine], kv[mine]
            kv_part = jnp.concatenate(
                [kv_part[i * deep : (i + 1) * deep] for i in range(fold)], axis=1
            ).astype(bf16)
            if n == 0:
                inbox[zone, tokens, r, :some_rows, :] = q_part
                inbox[zone, tokens, r, some_rows:, :] = kv_part
            else:
                outbox[n, g, r, :some_rows, :] = q_part
                outbox[n, g, r, some_rows:, :] = kv_part
        if n > 0:
            sent = pl.ds(parts[0], len(parts))
            remote(
                outbox.at[n, g, sent], inbox.at[zone, tokens, sent],
                send_m, recv_m.at[zone], at_zone(z),
            ).start()

    def share_keys(n):
        z = source(n)
        if n > 0:
            remote(inbox.at[z], inbox.at[z], send_m, recv_m.at[z], at_zone(zone)).wait_recv()
        for i in range(1, group):
            remote(
                inbox.at[z, :, :, pl.ds(some_rows, deep), :], kvbox.at[z, place],
                send_k.at[i - 1], recv_k.at[z, place], at_place(i),
            ).start()
        kvbox[z, place] = inbox[z, :, :, some_rows:, :]

    def keys_sent():
        remote(
            outbox.at[pl.ds(1, zones - 1)], outbox.at[pl.ds(1, zones - 1)],
            send_m, recv_m.at[zone], partner,
        ).wait_send()
        for i in range(1, group):
            every = inbox.at[:, :, :, pl.ds(some_rows, deep), :]
            remote(every, every, send_k.at[i - 1], recv_k.at[zone, place], partner).wait_send()

    def collect(n):
        z = source(n)
        q = jnp.concatenate(
            [
                inbox[z, t, r, :some_rows, :].astype(f32)
                for t in range(group)
                for r in range(halves)
            ],
            axis=0,
        )
        turned = q.T * (LOG2E * HEAD_DIM**-0.5)
        high = turned.astype(bf16)
        low = (turned - high.astype(f32)).astype(bf16)
        for h in range(heads):
            lanes = slice(h * span, (h + 1) * span)
            own = slice(h * HEAD_DIM, (h + 1) * HEAD_DIM)
            q_t[z, :HEAD_DIM, lanes] = high[own]
            q_t[z, HEAD_DIM : 2 * HEAD_DIM, lanes] = low[own]
        for i in range(1, group):
            owner = token_place(i)
            remote(
                kvbox.at[z, owner], kvbox.at[z, owner],
                send_k.at[i - 1], recv_k.at[z, owner], at_place(i),
            ).wait_recv()
        for t in range(group):
            parts = []
            for p in range(group):
                packed = [kvbox[z, p, t, r].astype(f32) for r in range(halves)]
                parts.append(
                    jnp.concatenate(
                        [
                            packed[r][:, i * ck2 : (i + 1) * ck2]
                            for r in range(halves)
                            for i in range(fold)
                        ],
                        axis=0,
                    )
                )
            keys = [p[:, :ck] for p in parts]
            values = [p[:, ck:] for p in parts]
            target = pl.ds(pl.multiple_of((z * group + t) * rows, rows), rows)
            k_aug[target, 0:128] = jnp.concatenate(keys + keys, axis=1).astype(bf16)
            turned = jnp.concatenate(keys + values, axis=1).T
            v_t[z * group + t] = turned[HEAD_DIM:].astype(bf16)

    def strict(t):
        key = lax.broadcasted_iota(jnp.int32, (rows, wide), 0) + t * rows
        query = lax.rem(lax.broadcasted_iota(jnp.int32, (rows, wide), 1), span)
        return key < query

    def attend(qz, kz, diagonal):
        after = None if diagonal else rest[qz]
        acc = None if diagonal else total[qz]
        logits = {}
        for t in reversed(range(group)):
            window = pl.ds(pl.multiple_of((kz * group + t) * rows, rows), rows)
            logits[t] = jnp.dot(
                k_aug[window, : 2 * HEAD_DIM + aug], q_t[qz], preferred_element_type=f32
            )
        kept = {}
        for t in reversed(range(group)):
            soft = logits[t]
            soft = jnp.maximum(soft, lax.log2(1.0 + lax.exp2(jnp.minimum(soft, 126.0))))
            if diagonal:
                soft = jnp.where(strict(t), soft, 0.0)
            kept[t] = jnp.dot(tri[...], soft.astype(bf16), preferred_element_type=f32)
        for t in reversed(range(group)):
            power = logits[t] + kept[t]
            if after is not None:
                power = power + after
            sticks = lax.exp2(power)
            if diagonal:
                sticks = jnp.where(strict(t), sticks, 0.0)
            more = jnp.dot(v_t[kz * group + t], sticks.astype(bf16), preferred_element_type=f32)
            acc = more if acc is None else acc + more
            after = kept[t][0:1, :] if after is None else after + kept[t][0:1, :]
        total[qz] = acc
        rest[qz] = after

    def send_head(s):
        return remote(
            head.at[pl.ds(s * rows, rows), :], arrived.at[sp], send_h, recv_h, {"sp": s}
        )

    def all_heads():
        others = pl.ds(0, (size - 1) * rows)
        return remote(head.at[others, :], head.at[others, :], send_h, recv_h, partner)

    def finish(qz):
        scaled = []
        for h in range(heads):
            some = total[qz, :, h * span : (h + 1) * span]
            scaled.append(
                some * lax.rsqrt(jnp.mean(some * some, axis=0, keepdims=True) + norm_eps)
            )
        lanes = pl.ds(pl.multiple_of(sp * cq, cq), cq) if cq % 128 == 0 else None
        gains = own_gain() if lanes is None else out_gain_ref[:, lanes]
        here = pl.ds(pl.multiple_of(qz * span, span), span)
        head[here, :] = (jnp.concatenate(scaled, axis=0).T * gains).astype(bf16)
        for t in range(group):
            s = qz * group + t

            @pl.when(s != sp)
            def _(s=s):
                send_head(s).start()

    def own_gain():
        both = out_gain_ref[:, pl.ds(pl.multiple_of(sp // 2 * 128, 128), 128)]
        return jnp.where(sp % 2 == 0, both[:, :cq], both[:, cq : 2 * cq])

    balanced = columns == group

    def lean_of(n):
        if not balanced:
            return 0
        return (core, 1, core, 1 - core)[n % 4]

    def weight(n, j, i):
        lean = lean_of(n)
        dx = j * (1 - lean) + i * lean
        dy = j * lean + i * (1 - lean)
        row = source(n) * group + lax.rem(place - dy + group, group)
        lane = lax.rem(column - dx + columns, columns) * cores + core
        return w_all.at[row, :, pl.ds(pl.multiple_of(lane * w_cols, w_cols), w_cols)]

    first_count = columns if not balanced else group
    second_count = group if not balanced else columns

    def at_first(n, j):
        lean = lean_of(n)
        return {
            "sp": zone * group + lax.rem(place + j * lean, group),
            "dp": lax.rem(column + j * (1 - lean), columns) * cores + core,
        }

    def at_second(n, i):
        lean = lean_of(n)
        return {
            "sp": zone * group + lax.rem(place + i * (1 - lean), group),
            "dp": lax.rem(column + i * lean, columns) * cores + core,
        }

    def w_core(n, j, i):
        remote(weight(n, j, i), weight(n, j, i), send_wc, recv_wc, partner).start()

    def w_second(n, j):
        for i in range(1, second_count):
            remote(
                weight(n, j, 0), weight(n, j, 0),
                send_wb.at[i - 1], recv_wb.at[n, j, i - 1], at_second(n, i),
            ).start()
        w_core(n, j, 0)

    def w_first(n):
        for j in range(1, first_count):
            remote(
                weight(n, 0, 0), weight(n, 0, 0),
                send_wa.at[j - 1], recv_wa.at[n, j - 1], at_first(n, j),
            ).start()
        w_second(n, 0)

    def w_sent():
        for n in range(zones):
            z = source(n)
            for way, peer, exists in send_outward(n):
                copy = remote(
                    weight(n, 0, 0), weight(n, 0, 0), send_wz.at[n, way], recv_wz.at[z], peer
                )

                @pl.when(exists)
                def _(copy=copy):
                    copy.wait_send()
        block = w_all.at[pl.ds(0, zones), :, pl.ds(0, w_cols)]
        for j in range(1, first_count):
            remote(block, block, send_wa.at[j - 1], recv_wa.at[0, j - 1], partner).wait_send()
        block = w_all.at[pl.ds(0, zones), :, pl.ds(0, first_count * w_cols)]
        for i in range(1, second_count):
            remote(block, block, send_wb.at[i - 1], recv_wb.at[0, 0, i - 1], partner).wait_send()

    def all_cores():
        block = w_all.at[:, :, pl.ds(0, columns * w_cols)]
        return remote(block, block, send_wc, recv_wc, partner)

    middle_zone = near > 0

    def wz_own(n):
        short = jnp.maximum(2 * near - 1, 0)
        for way, peer, exists in send_outward(0):
            fewer = above < below if way == 0 else below <= above
            last = jnp.where(fewer, short, zones - 1)
            copy = remote(
                weight(0, 0, 0), weight(0, 0, 0), send_wz.at[0, way], recv_wz.at[zone], peer
            )

            @pl.when(exists & (last == n))
            def _(copy=copy):
                copy.start()

    def wz_pass(n, now):
        z = source(n)

        @pl.when(now)
        def _():
            remote(
                weight(n, 0, 0), weight(n, 0, 0), send_wz.at[n, 0], recv_wz.at[z], at_zone(zone)
            ).wait_recv()
            for way, peer, exists in send_outward(n):
                copy = remote(
                    weight(n, 0, 0), weight(n, 0, 0), send_wz.at[n, way], recv_wz.at[z], peer
                )

                @pl.when(exists)
                def _(copy=copy):
                    copy.start()

    def w_first_event(n):
        for j in range(1, first_count):
            remote(
                weight(n, j, 0), weight(n, j, 0),
                send_wa.at[j - 1], recv_wa.at[n, j - 1], at_first(n, j),
            ).wait_recv()
            w_second(n, j)

    def w_second_event(n):
        for j in range(first_count):
            for i in range(1, second_count):
                remote(
                    weight(n, j, i), weight(n, j, i),
                    send_wb.at[i - 1], recv_wb.at[n, j, i - 1], at_second(n, i),
                ).wait_recv()
                w_core(n, j, i)

    def settle(n):
        for j in range(columns):
            z = source(n)
            remote(
                piece(z, cores * j), piece(z, cores * j + 1),
                send_c.at[j], recv_c.at[n, j], partner,
            ).wait_recv()

    def far(g, r):
        first = r * some_rows
        window = pl.ds(first, some_rows)
        return remote(
            x_ref.at[window, :], x_far.at[g - 1, window, :],
            send_y.at[g - 1, r], recv_y.at[g - 1, r], at_place(g),
        )

    def far_arrives(r):
        for g in range(1, group):
            far(g, r).wait_recv()
            normalize(x_far.at[g - 1], g, r * some_rows, some_rows)

    def far_project(n, parts):
        for g in range(1, group):
            project(n, g, parts)

    arrive(0)
    x_copy.wait()
    for r in range(halves):
        for g in range(1, group):
            far(g, r).start()
    own_weight.wait()
    wz_own(0)
    normalize(x_ref, 0, 0, rows)
    end_zone = jnp.logical_not(middle_zone)
    last = zones - 1
    def late(n):
        wz_pass(n, end_zone)
        w_first(n)

    def pass_on(n):
        wz_pass(n, middle_zone)

    plan = {
        "far": [(w_first, 0)],
        (1, 1): [(w_first_event, 1), (share_keys, 2), (share_keys, 3), (late, 2)],
        "projected": [(pass_on, 2)],
        "start": [(pass_on, 3), (late, 1), (w_first_event, 0)],
        (2, 1): [(w_second_event, 0)],
        (2, 2): [(late, 3), (w_second_event, 1), (w_first_event, 2)],
        (3, 3): [(w_first_event, 3), (w_second_event, 2)],
    }

    def run(slot):
        for event, k in plan.get(slot, ()):
            event(k)

    for n in range(1, last):
        arrive(n)
        wz_own(n)
        if n == 1:
            spread_columns(0)
    settle(0)
    project(0, 0)

    @pl.when(middle_zone)
    def _():
        arrive(last)
        wz_own(last)
        wz_pass(1, middle_zone)

    for n in range(1, last):
        if n == last - 1:
            @pl.when(end_zone)
            def _():
                arrive(last)
                wz_own(last)

        spread_columns(n)
        if n == 1:
            far_arrives(0)
            far_project(0, (0,))
        settle(n)
        project(n, 0)
        far_project(n, (0,))
        run(("early", n))
    far_arrives(1)
    run("far")
    for n in range(last):
        if n == 1:
            spread_columns(last)
        far_project(n, (1,))
    share_keys(0)
    run("shared")
    settle(last)
    for g in range(group):
        project(last, g)
    run("projected")

    for n in range(zones):
        if n == 0:
            share_keys(1)
            run("start")
        elif n > 3:
            share_keys(n)
            late(n)
            w_first_event(n)
        collect(n)
        a = source(n)
        upward = a > zone if n > 0 else None
        attend(a, a, True)
        if n == 0:
            tiles = [(a, a)]
        else:
            tiles = [(a, a)] + [
                (jnp.where(upward, a, a + m), jnp.where(upward, a - m, a)) for m in range(1, n + 1)
            ]
        for m, (qz, kz) in enumerate(tiles):
            if m > 0:
                attend(qz, kz, False)

            @pl.when(kz == 0)
            def _(qz=qz):
                finish(qz)

            run((n, m))
    for n in range(3, zones):
        w_second_event(n)
    mine = pltpu.make_async_copy(
        head.at[pl.ds(pl.multiple_of(sp * rows, rows), rows), :], arrived.at[sp], own_sem
    )
    mine.start()
    weights_sent()
    keys_sent()
    for r in range(halves):
        for g in range(1, group):
            far(g, r).wait_send()
    w_sent()
    mine.wait()
    all_heads().wait_recv()
    for s in range(size):
        joined[:, s * cq : (s + 1) * cq] = arrived[s]
    def multiply(c):
        for j in range(columns):
            lanes = pl.ds(pl.multiple_of((j * cores + c) * w_cols, w_cols), w_cols)
            out_ref[:, lanes] = jnp.dot(
                joined[...], w_all[:, :, lanes].reshape(size * cq, w_cols),
                preferred_element_type=f32,
            ).astype(bf16)

    multiply(core)
    all_cores().wait_recv()
    multiply(1 - core)
    all_cores().wait_send()
    all_heads().wait_send()


def layer(x, in_gain, wq, wk, wv, bias, out_gain, w_out, zones, group):
    rows, width = x.shape
    pieces = lax.axis_size("dp")
    columns = pieces // cores
    size = zones * group
    span = group * rows
    length = size * rows
    depth, cq = wq.shape
    ck2 = 2 * wk.shape[0]
    fold = cq // ck2
    heads = bias.shape[0]
    wide = heads * span
    some_rows = rows // halves
    deep = some_rows // fold
    dma = pltpu.SemaphoreType.DMA
    most = max(columns, group)
    return pl.pallas_call(
        functools.partial(layer_kernel, zones, group),
        out_shape=pltpu.VMEM((rows, width), bf16),
        in_specs=[ANY_SPEC] * 8,
        out_specs=VMEM_SPEC,
        scratch_shapes=[
            pltpu.VMEM(in_gain.shape, f32),
            pltpu.VMEM(wk.shape, bf16),
            pltpu.VMEM(wv.shape, bf16),
            pltpu.VMEM(bias.shape, f32),
            pltpu.VMEM(out_gain.shape, f32),
            pltpu.VMEM((rows, width), bf16),
            pltpu.VMEM((zones, pieces, depth + depth // 2, cq), bf16),
            pltpu.VMEM((group - 1, rows, width), bf16),
            pltpu.VMEM((group, 2, rows, width // 2), bf16),
            pltpu.VMEM((zones, group, halves, some_rows + deep, cq), bf16),
            pltpu.VMEM((zones, group, halves, some_rows + deep, cq), bf16),
            pltpu.VMEM((zones, group, group, halves, deep, cq), bf16),
            pltpu.VMEM((length, 256), bf16),
            pltpu.VMEM((size, HEAD_DIM, rows), bf16),
            pltpu.VMEM((zones, 2 * HEAD_DIM + aug, wide), bf16),
            pltpu.VMEM((zones, 1, wide), f32),
            pltpu.VMEM((zones, HEAD_DIM, wide), f32),
            pltpu.VMEM((rows, rows), bf16),
            pltpu.VMEM((size, w_out.shape[0], width), bf16),
            pltpu.VMEM((length, cq), bf16),
            pltpu.VMEM((size, rows, cq), bf16),
            pltpu.VMEM((rows, size * cq), bf16),
            dma, dma, dma, dma((5,)),
            dma((zones, 2)), dma((zones, chunks)),
            dma((columns - 1,)), dma((zones, columns - 1)),
            dma((columns,)), dma((zones, columns)),
            dma((group - 1, halves)), dma((group - 1, halves)),
            dma, dma((zones,)),
            dma((group - 1,)), dma((zones, group)),
            dma((zones, 2)), dma((zones,)),
            dma((most - 1,)), dma((zones, most - 1)),
            dma((most - 1,)), dma((zones, most, most - 1)),
            dma, dma,
            dma, dma,
        ],
        compiler_params=pltpu.CompilerParams(collective_id=0, has_side_effects=True),
        name="layer",
    )(x, in_gain, wq, wk, wv, bias, out_gain, w_out)


def body(inputs, in_gain, w_query, w_key, w_value, key_bias, out_gain, w_out):
    group = HEAD_DIM // w_key.shape[1]
    zones = lax.axis_size("sp") // group
    return layer(
        inputs[0], in_gain[None], w_query, w_key.T, w_value.T, key_bias[0].T,
        out_gain[None], w_out, zones, group,
    )[None]


def solution(mesh):
    placed = (
        P("dp", "sp", None),
        P(),
        P("dp", "sp"),
        P("dp", "sp"),
        P("dp", "sp"),
        P("dp", None, "sp"),
        P(),
        P("sp", "dp"),
    )
    return jax.shard_map(
        body, mesh=mesh, in_specs=placed, out_specs=P("dp", "sp", None), check_vma=False
    )
```
